128 devices in a mesh: sp: 32 (over z, y, core), tp: 4 (over x).
Axes of the slice: x: 4, y: 4, z: 4, core: 2. Of those that a mesh axis runs over, the one named last changes fastest.
Arguments:
- tokens: bfloat16 [12288, 2048], P('sp', 'tp'), may hold values from -6 to 6
- norm_gain: float32 [2048], replicated, may hold values from 0.1 to 1.9
- w_query_down: bfloat16 [2048, 512], replicated, may hold values from -0.125 to 0.125
- query_gain: float32 [512], replicated, may hold values from 0.1 to 1.9
- w_query_up: bfloat16 [512, 1536], P(None, 'tp'), may hold values from -0.25 to 0.25
- w_latent_down: bfloat16 [2048, 256], replicated, may hold values from -0.125 to 0.125
- latent_gain: float32 [256], replicated, may hold values from 0.1 to 1.9
- w_rotary_key: bfloat16 [2048, 32], replicated, may hold values from -0.125 to 0.125
- w_latent_up: bfloat16 [256, 2048], P(None, 'tp'), may hold values from -0.375 to 0.375
- query_head_gain: float32 [96], replicated, may hold values from 0.1 to 1.9
- key_head_gain: float32 [96], replicated, may hold values from 0.1 to 1.9
- w_pool_in: bfloat16 [2048, 1024], P(None, 'tp'), may hold values from -0.125 to 0.125
- w_pool_mix: bfloat16 [4, 256, 256], P('tp'), may hold values from -0.375 to 0.375
- pool_scale: float32 [1024], P('tp'), may hold values from 0.1 to 1.9
- w_attn_out: bfloat16 [1024, 2048], P('tp'), may hold values from -12 to 12
- w_pool_out: bfloat16 [1024, 2048], P('tp'), may hold values from -0.5 to 0.5
- w_gate_attn: bfloat16 [2048, 2048], P(None, 'tp'), may hold values from -0.125 to 0.125
- w_gate_pool: bfloat16 [2048, 2048], P(None, 'tp'), may hold values from -0.125 to 0.125
Outputs:
- mixed: bfloat16 [12288, 2048], P('sp', 'tp')
The draws below stay inside these ranges and needn't reach their ends.
All inputs are finite; a program needn't handle non-finite values.
Results may differ from the reference program's by a relative error of at most 0.02.
Values may be sent and summed in bfloat16 or wider, within the bound.
No kernel may reach another device: no remote copies, remote signals or barrier semaphores. Data moves between devices by JAX's collectives and lax.ppermute only.
A program may use at most 128 MiB of HBM per device.

```python
import math
import jax
import jax.numpy as jnp
from jax import lax

D = 2048
HEADS = 16
QUERY_RANK = 512
LATENT_RANK = 256
NOPE = 64
ROPE = 32
VALUE_DIM = 64
POOL_GROUPS = 4
POOL_GROUP = 256
POOL_WIDTH = 1024
TOKENS = 12288


def level_of(rng, extent, pieces, smallest, top_value):
    def one(dim, shards_of):
        steps = jax.random.uniform(jax.random.fold_in(jax.random.fold_in(rng, 6), dim), (shards_of,), jnp.float32, smallest / len(pieces), top_value / len(pieces))
        return jnp.repeat(jnp.exp(steps), extent[dim] // shards_of).reshape((-1,) + (1,) * (len(extent) - dim - 1))

    level = one(*pieces[0])
    for cut in pieces[1:]:
        level = level * one(*cut)
    return level


def centred(own_key, shape, deviation, most, split=(), held_as=jnp.bfloat16):
    result = jax.random.normal(own_key, shape, jnp.float32) * deviation
    if len(split) > 0:
        result = level_of(own_key, shape, split, -0.22, 0.18) * result
    return jnp.clip(result, min=-most, max=most).astype(held_as)


def setup_inputs(seed: int = 0) -> dict:
    streams_of = jax.random.split(jax.random.key(seed), 19)
    return {
        "tokens": centred(streams_of[0], (TOKENS, D), 1.0, 6.0, ((0, 32), (1, 4))),
        "norm_gain": jnp.clip(1.0 + 0.18 * jax.random.normal(streams_of[1], (D,), jnp.float32), 0.1, 1.9),
        "w_query_down": centred(streams_of[2], (D, QUERY_RANK), D ** -0.5, 0.125),
        "query_gain": jnp.clip(1.0 + 0.18 * jax.random.normal(streams_of[3], (QUERY_RANK,), jnp.float32), 0.1, 1.9),
        "w_query_up": centred(streams_of[4], (QUERY_RANK, HEADS * (NOPE + ROPE)), QUERY_RANK ** -0.5, 0.25, ((1, 4),)),
        "w_latent_down": centred(streams_of[5], (D, LATENT_RANK), D ** -0.5, 0.125),
        "latent_gain": jnp.clip(1.0 + 0.18 * jax.random.normal(streams_of[6], (LATENT_RANK,), jnp.float32), 0.1, 1.9),
        "w_rotary_key": centred(streams_of[7], (D, ROPE), D ** -0.5, 0.125),
        "w_latent_up": centred(streams_of[8], (LATENT_RANK, HEADS * (NOPE + VALUE_DIM)), LATENT_RANK ** -0.5, 0.375, ((1, 4),)),
        "query_head_gain": jnp.clip(1.0 + 0.18 * jax.random.normal(streams_of[9], (NOPE + ROPE,), jnp.float32), 0.1, 1.9),
        "key_head_gain": jnp.clip(1.0 + 0.18 * jax.random.normal(streams_of[10], (NOPE + ROPE,), jnp.float32), 0.1, 1.9),
        "w_pool_in": centred(streams_of[11], (D, POOL_WIDTH), D ** -0.5, 0.125, ((1, 4),)),
        "w_pool_mix": centred(streams_of[12], (POOL_GROUPS, POOL_GROUP, POOL_GROUP), POOL_GROUP ** -0.5, 0.375, ((0, 4),)),
        "pool_scale": jnp.clip(1.0 + 0.18 * jax.random.normal(streams_of[13], (POOL_WIDTH,), jnp.float32), 0.1, 1.9),
        "w_attn_out": centred(streams_of[14], (HEADS * VALUE_DIM, D), 2.0, 12.0, ((0, 4),)),
        "w_pool_out": centred(streams_of[15], (POOL_WIDTH, D), (POOL_WIDTH // 8) ** -0.5, 0.5, ((0, 4),)),
        "w_gate_attn": centred(streams_of[16], (D, D), D ** -0.5, 0.125, ((1, 4),)),
        "w_gate_pool": centred(streams_of[17], (D, D), D ** -0.5, 0.125, ((1, 4),)),
    }


eps = 1e-06
theta = 10000.0

def rms_scale(values, gain):
    values = values.astype(jnp.float32)
    return values * lax.rsqrt(lax.optimization_barrier(jnp.mean(values * values, axis=-1, keepdims=True)) + eps) * gain

def rotate(values, positions):
    half = values.shape[-1] // 2
    freqs = theta ** (-jnp.arange(half, dtype=jnp.float32) / half)
    angles = positions.astype(jnp.float32)[:, None] * freqs[None, :]
    cosine = jnp.cos(angles)[:, None, :]
    sine = jnp.sin(angles)[:, None, :]
    first = values[..., :half]
    second = values[..., half:]
    return jnp.concatenate([first * cosine - second * sine, first * sine + second * cosine], axis=-1)

def head_finish(values, gain, positions):
    normed = rms_scale(values, gain)
    return jnp.concatenate([normed[..., :NOPE], rotate(normed[..., NOPE:], positions)], axis=-1)

def reference(tokens, norm_gain, w_query_down, query_gain, w_query_up, w_latent_down, latent_gain, w_rotary_key, w_latent_up, query_head_gain, key_head_gain, w_pool_in, w_pool_mix, pool_scale, w_attn_out, w_pool_out, w_gate_attn, w_gate_pool):
    length = tokens.shape[0]
    bf = jnp.bfloat16
    positions = jnp.arange(length, dtype=jnp.int32)
    normed = rms_scale(tokens, norm_gain).astype(bf)
    query_latent = jnp.dot(normed, w_query_down, preferred_element_type=jnp.float32).astype(bf)
    query_normed = rms_scale(query_latent, query_gain).astype(bf)
    query_raw = jnp.dot(query_normed, w_query_up, preferred_element_type=jnp.float32).astype(bf)
    query_raw = query_raw.reshape(length, HEADS, NOPE + ROPE)
    query = (head_finish(query_raw, query_head_gain, positions) * (NOPE + ROPE) ** (-0.5)).astype(bf)
    latent = jnp.dot(normed, w_latent_down, preferred_element_type=jnp.float32).astype(bf)
    key_latent = rms_scale(latent, latent_gain).astype(bf)
    rotary_key = jnp.dot(normed, w_rotary_key, preferred_element_type=jnp.float32).astype(bf)
    keys_values = jnp.dot(key_latent, w_latent_up, preferred_element_type=jnp.float32).astype(bf)
    keys_values = keys_values.reshape(length, HEADS, NOPE + VALUE_DIM)
    key_raw = jnp.concatenate([keys_values[..., :NOPE], jnp.broadcast_to(rotary_key[:, None, :], (length, HEADS, ROPE))], axis=-1)
    key = head_finish(key_raw, key_head_gain, positions).astype(bf).astype(jnp.float32)
    values = keys_values[..., NOPE:].astype(jnp.float32)
    block = math.gcd(length, 256)
    query_blocks = query.reshape(length // block, block, HEADS, NOPE + ROPE)

    def attend(query_block):
        scores = jnp.einsum('qhd,khd->hqk', query_block.astype(jnp.float32), key)
        top = lax.optimization_barrier(jnp.max(scores, axis=-1, keepdims=True))
        expo = jnp.exp(scores - top)
        total = lax.optimization_barrier(jnp.sum(expo, axis=-1))
        rounded = lax.optimization_barrier(expo.astype(bf)).astype(jnp.float32)
        weighted = jnp.einsum('hqk,khv->qhv', rounded, values)
        return (weighted / jnp.transpose(total)[:, :, None]).astype(bf)
    attn_rows = lax.map(attend, query_blocks).reshape(length, HEADS * VALUE_DIM)
    pool_input = jnp.dot(normed, w_pool_in, preferred_element_type=jnp.float32).astype(bf)
    reach = 2 ** POOL_GROUPS // 2
    padded = jnp.pad(pool_input.astype(jnp.float32), ((reach, reach), (0, 0)))
    windows = jnp.power(2, jnp.arange(POOL_GROUPS, dtype=jnp.int32) + 1)
    channel_window = jnp.repeat(windows, POOL_GROUP)
    total = jnp.zeros((length, POOL_GROUPS * POOL_GROUP), jnp.float32)
    for shift in range(-reach, reach):
        inside = (shift >= -(channel_window // 2)) & (shift <= channel_window - channel_window // 2 - 1)
        total = total + jnp.where(inside[None, :], padded[reach + shift:reach + shift + length], 0.0)
    low = jnp.clip(positions[:, None] - channel_window[None, :] // 2, 0, length)
    high = jnp.clip(positions[:, None] + channel_window[None, :] - channel_window[None, :] // 2, 0, length)
    count = (high - low).astype(jnp.float32)
    pool_mixed = (total / count - pool_input.astype(jnp.float32)).astype(bf)
    pool_mixed = pool_mixed.reshape(length, POOL_GROUPS, POOL_GROUP)
    grouped = jnp.einsum('lgc,gcd->lgd', pool_mixed.astype(jnp.float32), w_pool_mix.astype(jnp.float32))
    pool_rows = (grouped.reshape(length, POOL_GROUPS * POOL_GROUP) * pool_scale).astype(bf)
    attn_branch = jnp.dot(attn_rows, w_attn_out, preferred_element_type=jnp.float32)
    pool_branch = jnp.dot(pool_rows, w_pool_out, preferred_element_type=jnp.float32)
    gate_attn = jax.nn.sigmoid(jnp.dot(normed, w_gate_attn, preferred_element_type=jnp.float32))
    gate_pool = jax.nn.sigmoid(jnp.dot(normed, w_gate_pool, preferred_element_type=jnp.float32))
    return (gate_attn * attn_branch + gate_pool * pool_branch).astype(bf)
```

```python
import functools
import math

import jax
import jax.numpy as jnp
from jax import lax
from jax.experimental import pallas as pl
from jax.experimental.pallas import tpu as pltpu
from jax.sharding import PartitionSpec as P

NOPE = 64
ROPE = 32
VALUE_DIM = 64
HEAD = NOPE + ROPE
LATENT = 256
REACH = 8
eps = 1e-06
theta = 10000.0
bf = jnp.bfloat16
f32 = jnp.float32

PAY = LATENT + ROPE + 16
ACC = VALUE_DIM + 16


def sp_of(z, y, c):
    return (z % 4) * 8 + (y % 4) * 2 + c


SITES = [(z, y, c) for z in range(4) for y in range(4) for c in range(2)]
SWAP = [(sp_of(z, y, c), sp_of(z, y, 1 - c)) for z, y, c in SITES]


def along(step, second):
    pairs = []
    for z, y, c in SITES:
        on_z = (c == 0) != second
        pairs.append((sp_of(z, y, c), sp_of(z + step, y, c) if on_z else sp_of(z, y + step, c)))
    return pairs


def ring(step):
    return [(i, (i + step) % 4) for i in range(4)]


def params(mib=56):
    return pltpu.CompilerParams(vmem_limit_bytes=mib * 2**20)


VM = pl.BlockSpec(memory_space=pltpu.VMEM)
SM = pl.BlockSpec(memory_space=pltpu.SMEM)


def front_kernel(ids, x0, x1, x2, x3a, x3b, gain, wl, wr, lgain, kgain, cos, sin, normed, pay):
    xs = [x0[...].astype(f32), x1[...].astype(f32), x2[...].astype(f32)]
    xs.append(jnp.concatenate([x3a[...], x3b[...]], axis=0).astype(f32))
    square = sum(jnp.sum(x * x, axis=-1, keepdims=True) for x in xs)
    scale = lax.rsqrt(square * (1.0 / 2048) + eps)
    lat = raw = None
    for j, x in enumerate(xs):
        at = pl.multiple_of(ids[j] * 512, 512)
        n = (x * scale * gain[:, pl.ds(at, 512)]).astype(bf)
        normed[:, pl.ds(at, 512)] = n
        a = jnp.dot(n, wl[pl.ds(at, 512), :], preferred_element_type=f32)
        b = jnp.dot(n, wr[pl.ds(at, 512), :], preferred_element_type=f32)
        lat = a if lat is None else lat + a
        raw = b if raw is None else raw + b
    lat = jnp.transpose(lat).astype(bf).astype(f32)
    lat = lat * lax.rsqrt(jnp.mean(lat * lat, axis=0, keepdims=True) + eps) * lgain[...]
    pay[:LATENT, :] = lat.astype(bf)
    raw = jnp.transpose(raw).astype(bf).astype(f32)
    total = jnp.sum(raw * raw, axis=0, keepdims=True)
    k = raw * kgain[...]
    first, second = k[:16], k[16:]
    pay[LATENT : LATENT + 16, :] = (first * cos[...] - second * sin[...]).astype(bf)
    pay[LATENT + 16 : LATENT + 32, :] = (first * sin[...] + second * cos[...]).astype(bf)
    pay[LATENT + 32 :, :] = jnp.broadcast_to(total, (16, total.shape[1])).astype(bf)


def query_kernel(normed, wqd, qgain, wqu, hgain, cos, sin, wpi, q, pool_in):
    n = normed[...]
    lat = jnp.dot(n, wqd[...], preferred_element_type=f32).astype(bf).astype(f32)
    lat = lat * lax.rsqrt(jnp.mean(lat * lat, axis=-1, keepdims=True) + eps) * qgain[...]
    raw = jnp.dot(lat.astype(bf), wqu[...], preferred_element_type=f32)
    raw = jnp.transpose(raw).astype(bf).astype(f32)
    for h in range(raw.shape[0] // HEAD):
        v = raw[h * HEAD : (h + 1) * HEAD]
        v = v * lax.rsqrt(jnp.mean(v * v, axis=0, keepdims=True) + eps) * hgain[...]
        v = v * (HEAD**-0.5 / math.log(2.0))
        first, second = v[NOPE : NOPE + 16], v[NOPE + 16 :]
        q[h, :NOPE, :] = v[:NOPE].astype(bf)
        q[h, NOPE : NOPE + 16, :] = (first * cos[...] - second * sin[...]).astype(bf)
        q[h, NOPE + 16 :, :] = (first * sin[...] + second * cos[...]).astype(bf)
    pool_in[...] = jnp.dot(n, wpi[...], preferred_element_type=f32).astype(bf)


def pool_kernel(ids, before, x, after, mix, scale, out, padded):
    rows = x.shape[0]
    length = ids[2]
    half = ids[1]
    padded[0:REACH, :] = before[...].astype(f32)
    padded[REACH : REACH + rows, :] = x[...].astype(f32)
    padded[REACH + rows :, :] = after[...].astype(f32)
    total = jnp.zeros((rows, x.shape[1]), f32)
    for shift in range(-REACH, REACH):
        inside = (shift >= -half) & (shift <= half - 1)
        total = total + jnp.where(inside, padded[REACH + shift : REACH + shift + rows, :], 0.0)
    at = ids[0] * rows + lax.broadcasted_iota(jnp.int32, (rows, 1), 0)
    count = (jnp.clip(at + half, 0, length) - jnp.clip(at - half, 0, length)).astype(f32)
    mixed = (total / count - padded[REACH : REACH + rows, :]).astype(bf)
    out[...] = (jnp.dot(mixed, mix[...], preferred_element_type=f32) * scale[...]).astype(bf)


def attend_kernel(*refs, pieces, seeded):
    q0, q1, wk, wv, gain = refs[:5]
    refs = refs[5:]
    n_in = sum(len(p) for p in pieces)
    blocks = refs[:n_in]
    refs = refs[n_in:]
    seeds, outs = (refs[:2], refs[2:]) if seeded else ((), refs)
    heads = q0.shape[0]
    half = q0.shape[2]
    at = 0
    for number, piece in enumerate(pieces):
        parts = [blocks[at + i] for i in range(len(piece))]
        at += len(piece)
        whole = parts[0][...] if len(parts) == 1 else jnp.concatenate([p[...] for p in parts], axis=0)
        keys = whole.shape[1]
        latent = whole[:LATENT]
        rope = whole[LATENT : LATENT + ROPE].astype(f32)
        square = whole[LATENT + ROPE :].astype(f32)[0:1]
        unrotated = jnp.dot(wk[...], latent, preferred_element_type=f32)
        values = jnp.dot(wv[...], latent, preferred_element_type=f32).astype(bf)
        row = lax.broadcasted_iota(jnp.int32, (16, keys), 0)
        ones = jnp.where(row == 0, 1.0, 0.0).astype(bf)
        for h in range(heads):
            k = unrotated[h * NOPE : (h + 1) * NOPE]
            scale = lax.rsqrt((jnp.sum(k * k, axis=0, keepdims=True) + square) * (1.0 / HEAD) + eps)
            key = jnp.concatenate([(k * gain[...] * scale).astype(bf), (rope * scale).astype(bf)], axis=0)
            query = jnp.concatenate([q0[h], q1[h]], axis=1)
            scores = lax.dot_general(key, query, (((0,), (0,)), ((), ())), preferred_element_type=f32)
            weights = jnp.exp2(scores).astype(bf)
            v = jnp.concatenate([values[h * VALUE_DIM : (h + 1) * VALUE_DIM], ones], axis=0)
            add = jnp.dot(v, weights, preferred_element_type=f32)
            for i in range(2):
                part = add[:, i * half : (i + 1) * half]
                if number > 0:
                    outs[i][h] += part
                elif seeded:
                    outs[i][h] = seeds[i][h] + part
                else:
                    outs[i][h] = part


def attend(q0, q1, wk, wv, gain, pieces, seeds):
    heads, _, half = q0.shape
    shape = jax.ShapeDtypeStruct((heads, ACC, half), f32)
    arrays = [a for p in pieces for a in p]
    keys = sum(p[0].shape[1] for p in pieces)
    kernel = functools.partial(
        attend_kernel, pieces=[[None] * len(p) for p in pieces], seeded=seeds is not None
    )
    return pl.pallas_call(
        kernel,
        in_specs=[VM] * (5 + len(arrays) + (2 if seeds else 0)),
        out_specs=[VM, VM],
        out_shape=[shape, shape],
        compiler_params=params(),
        cost_estimate=pl.CostEstimate(
            flops=keys * heads * 2 * half * 2 * 512,
            transcendentals=keys * heads * 2 * half,
            bytes_accessed=keys * PAY * 2,
        ),
        name="attend",
    )(q0, q1, wk, wv, gain, *arrays, *(seeds or ()))


def finish_kernel(mine, other, out):
    for h in range(mine.shape[0]):
        both = mine[h] + other[h]
        out[h * VALUE_DIM : (h + 1) * VALUE_DIM, :] = (
            both[:VALUE_DIM] / both[VALUE_DIM : VALUE_DIM + 1]
        ).astype(bf)


def merge_kernel(a0, a1, a2, a3, w0, w1, w2, w3, gate, pool, out):
    total = None
    for a, w in ((a0, w0), (a1, w1), (a2, w2), (a3, w3)):
        part = lax.dot_general(a[...], w[:256, :], (((0,), (0,)), ((), ())), preferred_element_type=f32)
        total = part if total is None else total + part
    out[...] = (gate[...] * total + pool[...]).astype(bf)


def call(kernel, ins, specs, shapes, name, flops, scratch=()):
    return pl.pallas_call(
        kernel,
        in_specs=specs,
        out_specs=jax.tree.map(lambda _: VM, shapes),
        out_shape=shapes,
        scratch_shapes=scratch,
        compiler_params=params(),
        cost_estimate=pl.CostEstimate(flops=flops, transcendentals=0, bytes_accessed=2**20),
        name=name,
    )(*ins)


def body(
    tokens,
    norm_gain,
    w_query_down,
    query_gain,
    w_query_up,
    w_latent_down,
    latent_gain,
    w_rotary_key,
    w_latent_up,
    query_head_gain,
    key_head_gain,
    w_pool_in,
    w_pool_mix,
    pool_scale,
    w_attn_out,
    w_pool_out,
    w_gate_attn,
    w_gate_pool,
):
    S = jax.ShapeDtypeStruct
    rows = tokens.shape[0]
    heads = w_query_up.shape[1] // HEAD
    length = rows * lax.axis_size("sp")
    here = lax.axis_index("sp")
    t = lax.axis_index("tp")

    x1 = lax.ppermute(tokens, "tp", ring(1))
    x2 = lax.ppermute(tokens, "tp", ring(-1))
    x3a = lax.ppermute(x1[: rows // 2], "tp", ring(1))
    x3b = lax.ppermute(x2[rows // 2 :], "tp", ring(-1))

    half = ROPE // 2
    freqs = theta ** (-jnp.arange(half, dtype=f32) / half)
    positions = (here * rows + jnp.arange(rows, dtype=jnp.int32)).astype(f32)
    angles = freqs[:, None] * positions[None, :]
    cos, sin = jnp.cos(angles), jnp.sin(angles)
    ids = jnp.stack([t, (t + 3) % 4, (t + 1) % 4, (t + 2) % 4]).astype(jnp.int32)
    up = w_latent_up.reshape(LATENT, heads, NOPE + VALUE_DIM)
    wk = jnp.transpose(up[:, :, :NOPE].reshape(LATENT, heads * NOPE))
    wv = jnp.transpose(up[:, :, NOPE:].reshape(LATENT, heads * VALUE_DIM))

    normed, pay = call(
        front_kernel,
        (ids, tokens, x1, x2, x3a, x3b, norm_gain[None, :], w_latent_down, w_rotary_key,
         latent_gain[:, None], key_head_gain[NOPE:, None], cos, sin),
        [SM] + [VM] * 12,
        [S((rows, 2048), bf), S((PAY, rows), bf)],
        "front",
        10**9,
    )

    def spread(x, second):
        plus = lax.ppermute(x, "sp", along(1, second))
        minus = lax.ppermute(x, "sp", along(-1, second))
        cut = PAY // 2
        far = (
            lax.ppermute(plus[:cut], "sp", along(1, second)),
            lax.ppermute(minus[cut:], "sp", along(-1, second)),
        )
        return plus, minus, far

    big, small = pay[:, :256], pay[:, 256:]
    big1 = spread(big, False)
    small1 = spread(small, True)

    q, pool_in = call(
        query_kernel,
        (normed, w_query_down, query_gain[None, :], w_query_up, query_head_gain[:, None], cos, sin, w_pool_in),
        [VM] * 8,
        [S((heads, HEAD, rows), bf), S((rows, 256), bf)],
        "query",
        2 * 10**9,
    )
    q_other = lax.ppermute(q, "sp", SWAP)

    def attend_on(pieces, seeds):
        return attend(q, q_other, wk, wv, key_head_gain[:NOPE, None], pieces, seeds)

    def joined(x, got):
        plus, minus, far = got
        return jnp.concatenate([x, plus, minus, jnp.concatenate(far, axis=0)], axis=1)

    big4, small4 = joined(big, big1), joined(small, small1)
    big2 = spread(big4, True)
    small2 = spread(small4, False)
    acc = attend_on([(big4,), (small4,)], None)
    acc = attend_on([(big2[0],), (big2[1],), (small2[0],), (small2[1],)], acc)
    acc = attend_on([big2[2], small2[2]], acc)

    count = lax.axis_size("sp")
    before = lax.ppermute(pool_in[rows - REACH :], "sp", [(i, i + 1) for i in range(count - 1)])
    after = lax.ppermute(pool_in[:REACH], "sp", [(i + 1, i) for i in range(count - 1)])
    pool_ids = jnp.stack([here, jnp.left_shift(1, t), jnp.int32(length)]).astype(jnp.int32)
    pool = call(
        pool_kernel,
        (pool_ids, before, pool_in, after, w_pool_mix[0], pool_scale[None, :]),
        [SM] + [VM] * 5,
        S((rows, 256), bf),
        "pool",
        10**8,
        [pltpu.VMEM((rows + 2 * REACH, 256), f32)],
    )
    pools = [pool] + [lax.ppermute(pool, "tp", ring(d)) for d in (1, 2, 3)]

    def columns(d):
        at = ((t + d) % 4) * 512
        return jnp.concatenate(
            [lax.dynamic_slice_in_dim(w, at, 512, axis=1) for w in (w_attn_out, w_pool_out)], axis=0
        )

    weights = [columns(0)] + [lax.ppermute(columns(d), "tp", ring(d)) for d in (1, 2, 3)]

    gate_attn = jax.nn.sigmoid(jnp.dot(normed, w_gate_attn, preferred_element_type=f32))
    gate_pool = jax.nn.sigmoid(jnp.dot(normed, w_gate_pool, preferred_element_type=f32))
    pool_branch = gate_pool * sum(
        jnp.dot(p, w[256:], preferred_element_type=f32) for p, w in zip(pools, weights)
    )

    other = lax.ppermute(acc[1], "sp", SWAP)
    attn = call(
        finish_kernel, (acc[0], other), [VM, VM], S((heads * VALUE_DIM, rows), bf), "finish", 10**7
    )
    attns = [attn] + [lax.ppermute(attn, "tp", ring(d)) for d in (1, 2, 3)]
    return call(
        merge_kernel,
        (*attns, *weights, gate_attn, pool_branch),
        [VM] * 10,
        S((rows, 512), bf),
        "merge",
        10**9,
    )


def solution(mesh):
    placed = (
        P("sp", "tp"),
        P(),
        P(),
        P(),
        P(None, "tp"),
        P(),
        P(),
        P(),
        P(None, "tp"),
        P(),
        P(),
        P(None, "tp"),
        P("tp", None, None),
        P("tp"),
        P("tp", None),
        P("tp", None),
        P(None, "tp"),
        P(None, "tp"),
    )
    return jax.shard_map(body, mesh=mesh, in_specs=placed, out_specs=P("sp", "tp"), check_vma=False)
```

```python
import functools
import math

import jax
import jax.numpy as jnp
from jax import lax
from jax.experimental import pallas as pl
from jax.experimental.pallas import tpu as pltpu
from jax.sharding import PartitionSpec as P


NOPE = 64
ROPE = 32
VALUE_DIM = 64
HEAD = NOPE + ROPE
LATENT = 256
REACH = 8
eps = 1e-06
theta = 10000.0
bf = jnp.bfloat16
f32 = jnp.float32

PAY = LATENT + ROPE + 16
ACC = VALUE_DIM + 16


def sp_of(z, y, c):
    return (z % 4) * 8 + (y % 4) * 2 + c


SITES = [(z, y, c) for z in range(4) for y in range(4) for c in range(2)]
SWAP = [(sp_of(z, y, c), sp_of(z, y, 1 - c)) for z, y, c in SITES]


def along(step, second):
    pairs = []
    for z, y, c in SITES:
        on_z = (c == 0) != second
        pairs.append((sp_of(z, y, c), sp_of(z + step, y, c) if on_z else sp_of(z, y + step, c)))
    return pairs


def ring(step):
    return [(i, (i + step) % 4) for i in range(4)]


def params(mib=56):
    return pltpu.CompilerParams(vmem_limit_bytes=mib * 2**20)


VM = pl.BlockSpec(memory_space=pltpu.VMEM)
SM = pl.BlockSpec(memory_space=pltpu.SMEM)


def gained(x, gain):
    return (x * gain).astype(bf)


def project_kernel(ids, *refs, count, seeded):
    xs, refs = refs[:count], refs[count:]
    gains, refs = refs[:count], refs[count:]
    weights, refs = refs[: 6 * count], refs[6 * count :]
    seeds, outs = (refs[:7], refs[7:]) if seeded else ((), refs)
    sums = [s[...] for s in seeds] if seeded else [None] * 7
    values = [x[...].astype(f32) for x in xs]
    square = sum(jnp.sum(x * x, axis=-1, keepdims=True) for x in values)
    square = jnp.broadcast_to(square, outs[0].shape)
    outs[0][...] = square if sums[0] is None else sums[0] + square
    ns = [gained(x, g[0]) for x, g in zip(values, gains)]
    for i in range(6):
        total = sums[i + 1]
        for k in range(count):
            w = weights[6 * k + i][...]
            if i == 1:
                part = lax.dot_general(w, ns[k], (((1,), (1,)), ((), ())), preferred_element_type=f32)
            else:
                part = jnp.dot(ns[k], w, preferred_element_type=f32)
            total = part if total is None else total + part
        outs[i + 1][...] = total


def last_piece(xa, xb, gain):
    x = jnp.concatenate([xa[...], xb[...]], axis=0).astype(f32)
    return x, gained(x, gain[0])


def front_kernel(ids, xa, xb, gain, wl, wr, square, lat0, raw0, lgain, kgain, cos, sin, pay, scale_out):
    x, n = last_piece(xa, xb, gain)
    total = square[...] + jnp.broadcast_to(jnp.sum(x * x, axis=-1, keepdims=True), square.shape)
    scale = lax.rsqrt(total * (1.0 / 2048) + eps)
    scale_out[...] = scale
    lat = lat0[...] + jnp.dot(n, wl[...], preferred_element_type=f32)
    lat = jnp.transpose(lat * scale[:, :1]).astype(bf).astype(f32)
    lat = lat * lax.rsqrt(jnp.mean(lat * lat, axis=0, keepdims=True) + eps) * lgain[...]
    pay[:LATENT, :] = lat.astype(bf)
    raw = raw0[...] + lax.dot_general(wr[...], n, (((1,), (1,)), ((), ())), preferred_element_type=f32)
    raw = (raw * jnp.transpose(scale)[:1]).astype(bf).astype(f32)
    total = jnp.sum(raw * raw, axis=0, keepdims=True)
    k = raw * kgain[...]
    first, second = k[:16], k[16:]
    pay[LATENT : LATENT + 16, :] = (first * cos[...] - second * sin[...]).astype(bf)
    pay[LATENT + 16 : LATENT + 32, :] = (first * sin[...] + second * cos[...]).astype(bf)
    pay[LATENT + 32 :, :] = jnp.broadcast_to(total, (16, total.shape[1])).astype(bf)


def query_kernel(ids, xa, xb, gain, wqd, wpi, scale, lat0, pool0, qgain, wqu, hgain, cos, sin, q, pool_in):
    _, n = last_piece(xa, xb, gain)
    s = scale[:, :1]
    pool_in[...] = ((pool0[...] + jnp.dot(n, wpi[...], preferred_element_type=f32)) * s).astype(bf)
    lat = (lat0[...] + jnp.dot(n, wqd[...], preferred_element_type=f32)) * s
    lat = lat.astype(bf).astype(f32)
    lat = lat * lax.rsqrt(jnp.mean(lat * lat, axis=-1, keepdims=True) + eps) * qgain[...]
    raw = jnp.dot(lat.astype(bf), wqu[...], preferred_element_type=f32)
    raw = jnp.transpose(raw).astype(bf).astype(f32)
    for h in range(raw.shape[0] // HEAD):
        v = raw[h * HEAD : (h + 1) * HEAD]
        v = v * lax.rsqrt(jnp.mean(v * v, axis=0, keepdims=True) + eps) * hgain[...]
        v = v * (HEAD**-0.5 / math.log(2.0))
        first, second = v[NOPE : NOPE + 16], v[NOPE + 16 :]
        q[h, :NOPE, :] = v[:NOPE].astype(bf)
        q[h, NOPE : NOPE + 16, :] = (first * cos[...] - second * sin[...]).astype(bf)
        q[h, NOPE + 16 :, :] = (first * sin[...] + second * cos[...]).astype(bf)


def gate_kernel(ids, xa, xb, gain, wa, wp, scale, a0, p0, gate_a, gate_p):
    _, n = last_piece(xa, xb, gain)
    s = scale[:, :1]
    gate_a[...] = jax.nn.sigmoid((a0[...] + jnp.dot(n, wa[...], preferred_element_type=f32)) * s)
    gate_p[...] = jax.nn.sigmoid((p0[...] + jnp.dot(n, wp[...], preferred_element_type=f32)) * s)


def columns_kernel(ids, wa, wp, *outs):
    for d in range(4):
        at = pl.multiple_of(ids[4 + d] * 512, 512)
        outs[d][:256, :] = wa[:, pl.ds(at, 512)]
        outs[d][256:, :] = wp[:, pl.ds(at, 512)]


def join_kernel(a, b, c, d, out):
    width = a.shape[1]
    for i, x in enumerate((a, b, c, d)):
        out[:, i * width : (i + 1) * width] = x[...]


def pool_merge_kernel(p0, p1, p2, p3, w0, w1, w2, w3, gate, out):
    total = None
    for p, w in ((p0, w0), (p1, w1), (p2, w2), (p3, w3)):
        part = jnp.dot(p[...], w[256:, :], preferred_element_type=f32)
        total = part if total is None else total + part
    out[...] = gate[...] * total


def pool_kernel(ids, before, x, after, mix, scale, out, padded):
    rows = x.shape[0]
    length = ids[2]
    half = ids[1]
    padded[0:REACH, :] = before[...].astype(f32)
    padded[REACH : REACH + rows, :] = x[...].astype(f32)
    padded[REACH + rows :, :] = after[...].astype(f32)
    total = jnp.zeros((rows, x.shape[1]), f32)
    for shift in range(-REACH, REACH):
        inside = (shift >= -half) & (shift <= half - 1)
        total = total + jnp.where(inside, padded[REACH + shift : REACH + shift + rows, :], 0.0)
    at = ids[0] * rows + lax.broadcasted_iota(jnp.int32, (rows, 1), 0)
    count = (jnp.clip(at + half, 0, length) - jnp.clip(at - half, 0, length)).astype(f32)
    mixed = (total / count - padded[REACH : REACH + rows, :]).astype(bf)
    out[...] = (jnp.dot(mixed, mix[...], preferred_element_type=f32) * scale[...]).astype(bf)


def attend_kernel(*refs, pieces, seeded):
    q0, q1, wk, wv, gain = refs[:5]
    refs = refs[5:]
    n_in = sum(len(p) for p in pieces)
    blocks = refs[:n_in]
    refs = refs[n_in:]
    seeds, outs = (refs[:2], refs[2:]) if seeded else ((), refs)
    heads = q0.shape[0]
    half = q0.shape[2]
    at = 0
    for number, piece in enumerate(pieces):
        parts = [blocks[at + i] for i in range(len(piece))]
        at += len(piece)
        whole = parts[0][...] if len(parts) == 1 else jnp.concatenate([p[...] for p in parts], axis=0)
        keys = whole.shape[1]
        latent = whole[:LATENT]
        rope = whole[LATENT : LATENT + ROPE].astype(f32)
        square = whole[LATENT + ROPE :].astype(f32)[0:1]
        unrotated = jnp.dot(wk[...], latent, preferred_element_type=f32)
        values = jnp.dot(wv[...], latent, preferred_element_type=f32).astype(bf)
        row = lax.broadcasted_iota(jnp.int32, (16, keys), 0)
        ones = jnp.where(row == 0, 1.0, 0.0).astype(bf)
        for h in range(heads):
            k = unrotated[h * NOPE : (h + 1) * NOPE]
            scale = lax.rsqrt((jnp.sum(k * k, axis=0, keepdims=True) + square) * (1.0 / HEAD) + eps)
            key = jnp.concatenate([(k * gain[...] * scale).astype(bf), (rope * scale).astype(bf)], axis=0)
            query = jnp.concatenate([q0[h], q1[h]], axis=1)
            scores = lax.dot_general(key, query, (((0,), (0,)), ((), ())), preferred_element_type=f32)
            weights = jnp.exp2(scores).astype(bf)
            v = jnp.concatenate([values[h * VALUE_DIM : (h + 1) * VALUE_DIM], ones], axis=0)
            add = jnp.dot(v, weights, preferred_element_type=f32)
            for i in range(2):
                part = add[:, i * half : (i + 1) * half]
                if number > 0:
                    outs[i][h] += part
                elif seeded:
                    outs[i][h] = seeds[i][h] + part
                else:
                    outs[i][h] = part


def attend(q0, q1, wk, wv, gain, pieces, seeds):
    heads, _, half = q0.shape
    shape = jax.ShapeDtypeStruct((heads, ACC, half), f32)
    arrays = [a for p in pieces for a in p]
    keys = sum(p[0].shape[1] for p in pieces)
    kernel = functools.partial(
        attend_kernel, pieces=[[None] * len(p) for p in pieces], seeded=seeds is not None
    )
    return pl.pallas_call(
        kernel,
        in_specs=[VM] * (5 + len(arrays) + (2 if seeds else 0)),
        out_specs=[VM, VM],
        out_shape=[shape, shape],
        compiler_params=params(),
        cost_estimate=pl.CostEstimate(
            flops=keys * heads * 2 * half * 2 * 512,
            transcendentals=keys * heads * 2 * half,
            bytes_accessed=keys * PAY * 2,
        ),
    )(q0, q1, wk, wv, gain, *arrays, *(seeds or ()))


def finish_kernel(mine, other, out):
    for h in range(mine.shape[0]):
        both = mine[h] + other[h]
        out[h * VALUE_DIM : (h + 1) * VALUE_DIM, :] = (
            both[:VALUE_DIM] / both[VALUE_DIM : VALUE_DIM + 1]
        ).astype(bf)


def merge_kernel(a0, a1, a2, a3, w0, w1, w2, w3, gate, pool, out):
    total = None
    for a, w in ((a0, w0), (a1, w1), (a2, w2), (a3, w3)):
        part = lax.dot_general(a[...], w[:256, :], (((0,), (0,)), ((), ())), preferred_element_type=f32)
        total = part if total is None else total + part
    out[...] = (gate[...] * total + pool[...]).astype(bf)


def call(kernel, ins, specs, shapes, flops, scratch=()):
    return pl.pallas_call(
        kernel,
        in_specs=specs,
        out_specs=jax.tree.map(lambda _: VM, shapes),
        out_shape=shapes,
        scratch_shapes=scratch,
        compiler_params=params(),
        cost_estimate=pl.CostEstimate(flops=flops, transcendentals=0, bytes_accessed=2**20),
    )(*ins)


def picked(kernel, ids, ins, shapes, flops):
    arrays, specs = [], []
    for a in ins:
        if isinstance(a, tuple):
            a, number, axis = a
            if axis is None:
                specs.append(pl.BlockSpec((1, 1, 512), lambda i, p, n=number: (p[n], 0, 0)))
            elif axis == 0:
                specs.append(pl.BlockSpec((512, a.shape[1]), lambda i, p, n=number: (p[n], 0)))
            else:
                specs.append(pl.BlockSpec((a.shape[0], 512), lambda i, p, n=number: (0, p[n])))
        else:
            specs.append(pl.BlockSpec(a.shape, lambda i, p, r=a.ndim: (0,) * r))
        arrays.append(a)
    return pl.pallas_call(
        kernel,
        grid_spec=pltpu.PrefetchScalarGridSpec(
            num_scalar_prefetch=1,
            grid=(1,),
            in_specs=specs,
            out_specs=[pl.BlockSpec(s.shape, lambda i, p, r=len(s.shape): (0,) * r) for s in shapes],
        ),
        out_shape=shapes,
        compiler_params=params(),
        cost_estimate=pl.CostEstimate(flops=flops, transcendentals=0, bytes_accessed=2**20),
    )(ids, *arrays)


def whole(
    tokens,
    norm_gain,
    w_query_down,
    query_gain,
    w_query_up,
    w_latent_down,
    latent_gain,
    w_rotary_key,
    w_latent_up,
    query_head_gain,
    key_head_gain,
    w_pool_in,
    w_pool_mix,
    pool_scale,
    w_attn_out,
    w_pool_out,
    w_gate_attn,
    w_gate_pool,
):
    S = jax.ShapeDtypeStruct
    rows = tokens.shape[0]
    heads = w_query_up.shape[1] // HEAD
    length = rows * lax.axis_size("sp")
    here = lax.axis_index("sp")
    t = lax.axis_index("tp")

    x1 = lax.ppermute(tokens, "tp", ring(1))
    x2 = lax.ppermute(tokens, "tp", ring(-1))
    xa = lax.ppermute(x1[: rows // 2], "tp", ring(1))
    xb = lax.ppermute(x2[rows // 2 :], "tp", ring(-1))

    half = ROPE // 2
    freqs = theta ** (-jnp.arange(half, dtype=f32) / half)
    positions = (here * rows + jnp.arange(rows, dtype=jnp.int32)).astype(f32)
    angles = freqs[:, None] * positions[None, :]
    cos, sin = jnp.cos(angles), jnp.sin(angles)
    ids = (t + jnp.array([0, 3, 1, 2, 0, 1, 2, 3], jnp.int32)) % 4
    up = w_latent_up.reshape(LATENT, heads, NOPE + VALUE_DIM)
    wk = jnp.transpose(up[:, :, :NOPE].reshape(LATENT, heads * NOPE))
    wv = jnp.transpose(up[:, :, NOPE:].reshape(LATENT, heads * VALUE_DIM))
    gain = norm_gain.reshape(4, 1, 512)
    wr = w_rotary_key.T

    def rows_of(n):
        return [(w_latent_down, n, 0), (wr, n, 1), (w_query_down, n, 0), (w_pool_in, n, 0),
                (w_gate_attn, n, 0), (w_gate_pool, n, 0)]

    sums = [S((rows, 128), f32), S((rows, 256), f32), S((ROPE, rows), f32), S((rows, 512), f32),
            S((rows, 256), f32), S((rows, 512), f32), S((rows, 512), f32)]
    own = picked(
        functools.partial(project_kernel, count=1, seeded=False),
        ids, [tokens, (gain, 0, None), *rows_of(0)], sums, 8 * 10**8,
    )
    near = picked(
        functools.partial(project_kernel, count=2, seeded=True),
        ids,
        [x1, x2, (gain, 1, None), (gain, 2, None), *rows_of(1), *rows_of(2), *own],
        sums, 16 * 10**8,
    )
    square, lat0, raw0, query0, pool0, attn0, gate0 = near
    last = [xa, xb, (gain, 3, None)]

    pay, scale = picked(
        front_kernel,
        ids,
        [*last, (w_latent_down, 3, 0), (wr, 3, 1), square, lat0, raw0, latent_gain[:, None],
         key_head_gain[NOPE:, None], cos, sin],
        [S((PAY, rows), bf), S((rows, 128), f32)],
        3 * 10**8,
    )

    cut = PAY // 2
    a1 = lax.ppermute(pay, "sp", along(1, False))
    a2 = lax.ppermute(pay, "sp", along(-1, False))
    a3 = lax.ppermute(pay, "sp", along(2, False))

    q, pool_in = picked(
        query_kernel,
        ids,
        [*last, (w_query_down, 3, 0), (w_pool_in, 3, 0), scale, query0, pool0, query_gain[None, :],
         w_query_up, query_head_gain[:, None], cos, sin],
        [S((heads, HEAD, rows), bf), S((rows, 256), bf)],
        10**9,
    )
    q_other = lax.ppermute(q, "sp", SWAP)

    def attend_on(pieces, seeds):
        return attend(q, q_other, wk, wv, key_head_gain[:NOPE, None], pieces, seeds)

    line = call(join_kernel, (pay, a1, a2, a3), [VM] * 4, S((PAY, 4 * rows), bf), 10**7)
    b1 = lax.ppermute(line, "sp", along(1, True))
    b2 = lax.ppermute(line, "sp", along(-1, True))
    b3 = lax.ppermute(b1[:cut], "sp", along(1, True))
    b4 = lax.ppermute(b2[cut:], "sp", along(-1, True))
    acc = attend_on([[line]], None)
    acc = attend_on([[b1], [b2]], acc)
    acc = attend_on([[b3, b4]], acc)

    count = lax.axis_size("sp")
    before = lax.ppermute(pool_in[rows - REACH :], "sp", [(i, i + 1) for i in range(count - 1)])
    after = lax.ppermute(pool_in[:REACH], "sp", [(i + 1, i) for i in range(count - 1)])
    pool_ids = jnp.stack([here, jnp.left_shift(1, t), jnp.int32(length)]).astype(jnp.int32)
    pool = call(
        pool_kernel,
        (pool_ids, before, pool_in, after, w_pool_mix[0], pool_scale[None, :]),
        [SM] + [VM] * 5,
        S((rows, 256), bf),
        10**8,
        [pltpu.VMEM((rows + 2 * REACH, 256), f32)],
    )
    pools = [pool] + [lax.ppermute(pool, "tp", ring(d)) for d in (1, 2, 3)]

    weights = call(columns_kernel, (ids, w_attn_out, w_pool_out), [SM, VM, VM], [S((512, 512), bf)] * 4, 10**7)
    weights = [weights[0]] + [lax.ppermute(weights[d], "tp", ring(d)) for d in (1, 2, 3)]

    gate_attn, gate_pool = picked(
        gate_kernel,
        ids,
        [*last, (w_gate_attn, 3, 0), (w_gate_pool, 3, 0), scale, attn0, gate0],
        [S((rows, 512), f32)] * 2,
        5 * 10**8,
    )
    pool_branch = call(pool_merge_kernel, (*pools, *weights, gate_pool), [VM] * 9, S((rows, 512), f32), 10**9)

    other = lax.ppermute(acc[1], "sp", SWAP)
    attn = call(finish_kernel, (acc[0], other), [VM, VM], S((heads * VALUE_DIM, rows), bf), 10**7)
    attns = [attn] + [lax.ppermute(attn, "tp", ring(d)) for d in (1, 2, 3)]
    return call(merge_kernel, (*attns, *weights, gate_attn, pool_branch), [VM] * 10, S((rows, 512), bf), 10**9)


def solution(mesh):
    placed = (
        P("sp", "tp"),
        P(),
        P(),
        P(),
        P(None, "tp"),
        P(),
        P(),
        P(),
        P(None, "tp"),
        P(),
        P(),
        P(None, "tp"),
        P("tp", None, None),
        P("tp"),
        P("tp", None),
        P("tp", None),
        P(None, "tp"),
        P(None, "tp"),
    )
    return jax.shard_map(whole, mesh=mesh, in_specs=placed, out_specs=P("sp", "tp"), check_vma=False)
```

```python
import functools
import math

import jax
import jax.numpy as jnp
from jax import lax
from jax.experimental import pallas as pl
from jax.experimental.pallas import tpu as pltpu
from jax.sharding import PartitionSpec as P


NOPE = 64
ROPE = 32
VALUE_DIM = 64
HEAD = NOPE + ROPE
LATENT = 256
REACH = 8
eps = 1e-06
theta = 10000.0
bf = jnp.bfloat16
f32 = jnp.float32

PAY = LATENT + ROPE + 16
ACC = VALUE_DIM + 16


def sp_of(z, y, c):
    return (z % 4) * 8 + (y % 4) * 2 + c


SITES = [(z, y, c) for z in range(4) for y in range(4) for c in range(2)]
SWAP = [(sp_of(z, y, c), sp_of(z, y, 1 - c)) for z, y, c in SITES]


def along(step, second):
    pairs = []
    for z, y, c in SITES:
        on_z = (c == 0) != second
        pairs.append((sp_of(z, y, c), sp_of(z + step, y, c) if on_z else sp_of(z, y + step, c)))
    return pairs


def ring(step):
    return [(i, (i + step) % 4) for i in range(4)]


def params(mib=56):
    return pltpu.CompilerParams(vmem_limit_bytes=mib * 2**20)


VM = pl.BlockSpec(memory_space=pltpu.VMEM)
SM = pl.BlockSpec(memory_space=pltpu.SMEM)


def gained(x, gain):
    return (x * gain).astype(bf)


def project_kernel(ids, *refs, first, count, seeded):
    xs, refs = refs[:count], refs[count:]
    gain, weights, refs = refs[0], refs[1:7], refs[7:]
    refs, (sems, *slots) = refs[:-7], refs[-7:]
    seeds, outs = (refs[:7], refs[7:]) if seeded else ((), refs[-7:])
    ats = [pl.multiple_of(ids[first + k] * 512, 512) for k in range(count)]
    copies = []
    for i, w in enumerate(weights):
        for k, at in enumerate(ats):
            source = w.at[:, pl.ds(at, 512)] if i == 1 else w.at[pl.ds(at, 512), :]
            copies.append(pltpu.make_async_copy(source, slots[i].at[k], sems.at[i, k]))
            copies[-1].start()
    values = [x[...].astype(f32) for x in xs]
    square = sum(jnp.sum(x * x, axis=-1, keepdims=True) for x in values)
    square = jnp.broadcast_to(square, outs[0].shape)
    outs[0][...] = seeds[0][...] + square if seeded else square
    ns = [gained(x, gain[:, pl.ds(at, 512)]) for x, at in zip(values, ats)]
    for i in range(6):
        total = seeds[i + 1][...] if seeded else None
        for k, n in enumerate(ns):
            copies[i * count + k].wait()
            part = product(n, slots[i][k], i == 1)
            total = part if total is None else total + part
        outs[i + 1][...] = total


def product(n, w, turned):
    if turned:
        return lax.dot_general(w, n, (((1,), (1,)), ((), ())), preferred_element_type=f32)
    return jnp.dot(n, w, preferred_element_type=f32)


def rows_at(w, at):
    return w[pl.ds(at, 512), :]


def last_piece(ids, x, gain):
    at = pl.multiple_of(ids[3] * 512, 512)
    x = x[...].astype(f32)
    return x, gained(x, gain[:, pl.ds(at, 512)]), at


def front_kernel(ids, x, gain, wl, wr, square, lat0, raw0, gains, cos, sin, pay, scale_out):
    x, n, at = last_piece(ids, x, gain)
    lgain, kgain = gains[:LATENT], gains[LATENT + NOPE : LATENT + HEAD]
    total = square[...] + jnp.broadcast_to(jnp.sum(x * x, axis=-1, keepdims=True), square.shape)
    scale = lax.rsqrt(total * (1.0 / 2048) + eps)
    scale_out[...] = scale
    lat = lat0[...] + product(n, rows_at(wl, at), False)
    lat = jnp.transpose(lat * scale[:, :1]).astype(bf).astype(f32)
    lat = lat * lax.rsqrt(jnp.mean(lat * lat, axis=0, keepdims=True) + eps) * lgain
    pay[:LATENT, :] = lat.astype(bf)
    raw = raw0[...] + product(n, wr[:, pl.ds(at, 512)], True)
    raw = (raw * jnp.transpose(scale)[:1]).astype(bf).astype(f32)
    total = jnp.sum(raw * raw, axis=0, keepdims=True)
    k = raw * kgain
    first, second = k[:16], k[16:]
    pay[LATENT : LATENT + 16, :] = (first * cos[...] - second * sin[...]).astype(bf)
    pay[LATENT + 16 : LATENT + 32, :] = (first * sin[...] + second * cos[...]).astype(bf)
    pay[LATENT + 32 :, :] = jnp.broadcast_to(total, (16, total.shape[1])).astype(bf)


def query_kernel(ids, x, gain, wqd, wpi, scale, lat0, pool0, qgain, wqu, gains, cos, sin, q, pool_in, inner, outer):
    _, n, at = last_piece(ids, x, gain)
    hgain = gains[LATENT + HEAD : LATENT + 2 * HEAD]
    s = scale[:, :1]
    pooled = (pool0[...] + product(n, rows_at(wpi, at), False)) * s
    pool_in[...] = pooled.astype(bf)
    head, end = pooled[:REACH], pooled[pooled.shape[0] - REACH :]
    on_first = ids[8] % 2 == 0
    inner[...] = jnp.where(on_first, end, head).astype(bf)
    outer[...] = jnp.where(on_first, head, end).astype(bf)
    lat = (lat0[...] + product(n, rows_at(wqd, at), False)) * s
    lat = lat.astype(bf).astype(f32)
    lat = lat * lax.rsqrt(jnp.mean(lat * lat, axis=-1, keepdims=True) + eps) * qgain[...]
    raw = jnp.dot(lat.astype(bf), wqu[...], preferred_element_type=f32)
    raw = jnp.transpose(raw).astype(bf).astype(f32)
    for h in range(raw.shape[0] // HEAD):
        v = raw[h * HEAD : (h + 1) * HEAD]
        v = v * lax.rsqrt(jnp.mean(v * v, axis=0, keepdims=True) + eps) * hgain
        v = v * (HEAD**-0.5 / math.log(2.0))
        first, second = v[NOPE : NOPE + 16], v[NOPE + 16 :]
        q[h, :NOPE, :] = v[:NOPE].astype(bf)
        q[h, NOPE : NOPE + 16, :] = (first * cos[...] - second * sin[...]).astype(bf)
        q[h, NOPE + 16 :, :] = (first * sin[...] + second * cos[...]).astype(bf)


def gate_kernel(ids, x, gain, wa, wp, scale, a0, p0, gate_a, gate_p):
    _, n, at = last_piece(ids, x, gain)
    s = scale[:, :1]
    gate_a[...] = jax.nn.sigmoid((a0[...] + product(n, rows_at(wa, at), False)) * s)
    gate_p[...] = jax.nn.sigmoid((p0[...] + product(n, rows_at(wp, at), False)) * s)


def join_kernel(a, b, c, d, out):
    width = a.shape[1]
    for i, x in enumerate((a, b, c, d)):
        out[:, i * width : (i + 1) * width] = x[...]


def pool_merge_kernel(pool, w0, w1, w2, w3, gate, out):
    total = jnp.dot(pool[...], w0[256:, :], preferred_element_type=f32)
    for w in (w1, w2, w3):
        p = jnp.concatenate([w[512:, :256], w[512:, 256:]], axis=0)
        total = total + jnp.dot(p, w[256:512, :], preferred_element_type=f32)
    out[...] = gate[...] * total


def pack_kernel(ids, inner, x, outer, mix, scale, wa, wp, pool, own, s1, s2, s3, padded):
    rows = x.shape[0]
    half, length = ids[9], ids[10]
    on_first = ids[8] % 2 == 0
    inner, outer = inner[...].astype(f32), outer[...].astype(f32)
    padded[0:REACH, :] = jnp.where(on_first, outer, inner)
    padded[REACH : REACH + rows, :] = x[...].astype(f32)
    padded[REACH + rows :, :] = jnp.where(on_first, inner, outer)
    total = jnp.zeros((rows, x.shape[1]), f32)
    for shift in range(-REACH, REACH):
        inside = (shift >= -half) & (shift <= half - 1)
        total = total + jnp.where(inside, padded[REACH + shift : REACH + shift + rows, :], 0.0)
    at = ids[8] * rows + lax.broadcasted_iota(jnp.int32, (rows, 1), 0)
    count = (jnp.clip(at + half, 0, length) - jnp.clip(at - half, 0, length)).astype(f32)
    mixed = (total / count - padded[REACH : REACH + rows, :]).astype(bf)
    out = (jnp.dot(mixed, mix[...], preferred_element_type=f32) * scale[...]).astype(bf)
    pool[...] = out
    for d, s in enumerate((own, s1, s2, s3)):
        at = pl.multiple_of(ids[4 + d] * 512, 512)
        s[:256, :] = wa[:, pl.ds(at, 512)]
        s[256:512, :] = wp[:, pl.ds(at, 512)]
        if d > 0:
            s[512:, :256] = out[: rows // 2]
            s[512:, 256:] = out[rows // 2 :]


def attend_kernel(*refs, pieces, seeded):
    q0, q1, up, gains = refs[:4]
    refs = refs[4:]
    gain = gains[LATENT : LATENT + NOPE]
    n_in = sum(len(p) for p in pieces)
    blocks = refs[:n_in]
    refs = refs[n_in:]
    seeds, outs = (refs[:2], refs[2:]) if seeded else ((), refs)
    heads = q0.shape[0]
    half = q0.shape[2]
    at = 0
    for number, piece in enumerate(pieces):
        parts = [blocks[at + i] for i in range(len(piece))]
        at += len(piece)
        whole = parts[0][...] if len(parts) == 1 else jnp.concatenate([p[...] for p in parts], axis=0)
        keys = whole.shape[1]
        latent = whole[:LATENT]
        rope = whole[LATENT : LATENT + ROPE].astype(f32)
        square = whole[LATENT + ROPE :].astype(f32)[0:1]
        expanded = lax.dot_general(up[...], latent, (((0,), (0,)), ((), ())), preferred_element_type=f32)
        row = lax.broadcasted_iota(jnp.int32, (16, keys), 0)
        ones = jnp.where(row == 0, 1.0, 0.0).astype(bf)
        for h in range(heads):
            k = expanded[h * 128 : h * 128 + NOPE]
            scale = lax.rsqrt((jnp.sum(k * k, axis=0, keepdims=True) + square) * (1.0 / HEAD) + eps)
            key = jnp.concatenate([(k * gain * scale).astype(bf), (rope * scale).astype(bf)], axis=0)
            query = jnp.concatenate([q0[h], q1[h]], axis=1)
            scores = lax.dot_general(key, query, (((0,), (0,)), ((), ())), preferred_element_type=f32)
            weights = jnp.exp2(scores).astype(bf)
            v = jnp.concatenate([expanded[h * 128 + NOPE : (h + 1) * 128].astype(bf), ones], axis=0)
            add = jnp.dot(v, weights, preferred_element_type=f32)
            for i in range(2):
                part = add[:, i * half : (i + 1) * half]
                if number > 0:
                    outs[i][h] += part
                elif seeded:
                    outs[i][h] = seeds[i][h] + part
                else:
                    outs[i][h] = part


def attend(q0, q1, up, gains, pieces, seeds):
    heads, _, half = q0.shape
    shape = jax.ShapeDtypeStruct((heads, ACC, half), f32)
    arrays = [a for p in pieces for a in p]
    keys = sum(p[0].shape[1] for p in pieces)
    kernel = functools.partial(
        attend_kernel, pieces=[[None] * len(p) for p in pieces], seeded=seeds is not None
    )
    return call(
        kernel,
        None,
        [q0, q1, up, gains, *[resident(a) for a in (*arrays, *(seeds or ()))]],
        [kept(shape), kept(shape)],
        keys * heads * 2 * half * 2 * 512,
        mib=28,
        transcendentals=keys * heads * 2 * half,
    )


def finish_kernel(mine, other, out):
    for h in range(mine.shape[0]):
        both = mine[h] + other[h]
        out[h * VALUE_DIM : (h + 1) * VALUE_DIM, :] = (
            both[:VALUE_DIM] / both[VALUE_DIM : VALUE_DIM + 1]
        ).astype(bf)


def merge_kernel(a0, a1, a2, a3, w0, w1, w2, w3, gate, pool, out):
    total = None
    for a, w in ((a0, w0), (a1, w1), (a2, w2), (a3, w3)):
        part = lax.dot_general(a[...], w[:256, :], (((0,), (0,)), ((), ())), preferred_element_type=f32)
        total = part if total is None else total + part
    out[...] = (gate[...] * total + pool[...]).astype(bf)


def resident(x):
    return pltpu.with_memory_space_constraint(x, pltpu.VMEM)


def kept(s):
    return pltpu.VMEM(s.shape, s.dtype)


def call(kernel, ids, ins, shapes, flops, scratch=(), mib=16, transcendentals=0, apart=()):
    first = [] if ids is None else [ids]
    ins = [pltpu.with_memory_space_constraint(x, pltpu.HBM) if i in apart else x for i, x in enumerate(ins)]
    return pl.pallas_call(
        kernel,
        in_specs=[SM] * len(first)
        + [pl.BlockSpec(memory_space=pltpu.HBM) if i in apart else VM for i in range(len(ins))],
        out_specs=jax.tree.map(lambda _: VM, shapes),
        out_shape=shapes,
        scratch_shapes=scratch,
        compiler_params=params(mib),
        cost_estimate=pl.CostEstimate(flops=flops, transcendentals=transcendentals, bytes_accessed=2**20),
    )(*first, *ins)


def whole(
    tokens,
    norm_gain,
    w_query_down,
    query_gain,
    w_query_up,
    w_latent_down,
    latent_gain,
    w_rotary_key,
    w_latent_up,
    query_head_gain,
    key_head_gain,
    w_pool_in,
    w_pool_mix,
    pool_scale,
    w_attn_out,
    w_pool_out,
    w_gate_attn,
    w_gate_pool,
):
    S = jax.ShapeDtypeStruct
    rows = tokens.shape[0]
    heads = w_query_up.shape[1] // HEAD
    length = rows * lax.axis_size("sp")
    here = lax.axis_index("sp")
    t = lax.axis_index("tp")

    x1 = lax.ppermute(tokens, "tp", ring(1))
    x2 = lax.ppermute(tokens, "tp", ring(-1))
    x3 = lax.ppermute(tokens, "tp", ring(2))

    half = ROPE // 2
    freqs = theta ** (-jnp.arange(half, dtype=f32) / half)
    positions = (here * rows + jnp.arange(rows, dtype=jnp.int32)).astype(f32)
    angles = freqs[:, None] * positions[None, :]
    cos, sin = jnp.cos(angles), jnp.sin(angles)
    ids = jnp.concatenate(
        [
            (t + jnp.array([0, 3, 1, 2, 0, 1, 2, 3], jnp.int32)) & 3,
            jnp.stack([here, jnp.left_shift(1, t), jnp.int32(length)]).astype(jnp.int32),
        ]
    )
    gains = jnp.concatenate([latent_gain, key_head_gain, query_head_gain])[:, None]
    gain = norm_gain[None, :]
    wr = w_rotary_key.T

    sums = [S((rows, 128), f32), S((rows, 256), f32), S((ROPE, rows), f32), S((rows, 512), f32),
            S((rows, 256), f32), S((rows, 512), f32), S((rows, 512), f32)]
    projections = [w_latent_down, wr, w_query_down, w_pool_in, w_gate_attn, w_gate_pool]

    def slots(count):
        shapes = [(count, 512, w.shape[1]) for w in projections]
        shapes[1] = (count, ROPE, 512)
        return [pltpu.SemaphoreType.DMA((6, count))] + [pltpu.VMEM(s, bf) for s in shapes]

    own = call(
        functools.partial(project_kernel, first=0, count=1, seeded=False),
        ids, [tokens, gain, *projections, gains, cos, sin], [kept(s) for s in sums], 8 * 10**8,
        slots(1), apart=range(2, 11),
    )
    near = call(
        functools.partial(project_kernel, first=1, count=2, seeded=True),
        ids, [resident(x1), resident(x2), gain, *projections, *[resident(s) for s in own]],
        [kept(s) for s in sums[:3]] + sums[3:], 16 * 10**8,
        slots(2), apart=range(3, 9),
    )
    square, lat0, raw0, query0, pool0, attn0, gate0 = near

    pay, scale = call(
        front_kernel,
        ids,
        [resident(x3), gain, w_latent_down, wr, resident(square), resident(lat0), resident(raw0), gains, cos, sin],
        [kept(S((PAY, rows), bf)), S((rows, 128), f32)],
        3 * 10**8,
    )

    a1 = lax.ppermute(pay, "sp", along(1, False))
    a2 = lax.ppermute(pay, "sp", along(-1, False))
    a3 = lax.ppermute(pay, "sp", along(2, False))

    q, pool_in, inner, outer = call(
        query_kernel,
        ids,
        [x3, gain, w_query_down, w_pool_in, scale, query0, pool0, query_gain[None, :],
         w_query_up, gains, cos, sin],
        [S((heads, HEAD, rows), bf), S((rows, 256), bf), S((REACH, 256), bf), S((REACH, 256), bf)],
        10**9,
    )
    q_other = lax.ppermute(q, "sp", SWAP)
    inner = lax.ppermute(inner, "sp", SWAP)
    count = lax.axis_size("sp")
    outer = lax.ppermute(outer, "sp", [(i, i - 1 + 2 * (i % 2)) for i in range(1, count - 1)])

    def attend_on(pieces, seeds):
        return attend(q, q_other, w_latent_up, gains, pieces, seeds)

    line = call(join_kernel, None, [resident(x) for x in (pay, a1, a2, a3)], kept(S((PAY, 4 * rows), bf)), 10**7)
    b1 = lax.ppermute(line, "sp", along(1, True))
    b2 = lax.ppermute(line, "sp", along(-1, True))
    cut = PAY // 2
    b3 = lax.ppermute(b1[:cut], "sp", along(1, True))
    b4 = lax.ppermute(b2[cut:], "sp", along(-1, True))

    pool, own_w, *packs = call(
        pack_kernel,
        ids,
        [inner, pool_in, outer, w_pool_mix[0], pool_scale[None, :], w_attn_out, w_pool_out],
        [S((rows, 256), bf), S((512, 512), bf)] + [S((704, 512), bf)] * 3,
        10**8,
        [pltpu.VMEM((rows + 2 * REACH, 256), f32)],
    )
    weights = [own_w] + [lax.ppermute(packs[d - 1], "tp", ring(d)) for d in (1, 2, 3)]

    acc = attend_on([[line]], None)
    acc = attend_on([[b1], [b2]], acc)
    acc = attend_on([[b3, b4]], acc)

    gate_attn, gate_pool = call(
        gate_kernel,
        ids,
        [x3, gain, w_gate_attn, w_gate_pool, scale, attn0, gate0],
        [kept(S((rows, 512), f32))] * 2,
        5 * 10**8,
    )
    pool_branch = call(pool_merge_kernel, None, [pool, *weights, resident(gate_pool)], kept(S((rows, 512), f32)), 10**9)

    other = lax.ppermute(acc[1], "sp", SWAP)
    attn = call(finish_kernel, None, [resident(acc[0]), resident(other)], kept(S((heads * VALUE_DIM, rows), bf)), 10**7)
    attns = [attn] + [lax.ppermute(attn, "tp", ring(d)) for d in (1, 2, 3)]
    return call(
        merge_kernel, None, [*[resident(a) for a in attns], *weights, resident(gate_attn), resident(pool_branch)], S((rows, 512), bf), 10**9
    )


def solution(mesh):
    placed = (
        P("sp", "tp"),
        P(),
        P(),
        P(),
        P(None, "tp"),
        P(),
        P(),
        P(),
        P(None, "tp"),
        P(),
        P(),
        P(None, "tp"),
        P("tp", None, None),
        P("tp"),
        P("tp", None),
        P("tp", None),
        P(None, "tp"),
        P(None, "tp"),
    )
    return jax.shard_map(whole, mesh=mesh, in_specs=placed, out_specs=P("sp", "tp"), check_vma=False)
```

```python
import functools
import math

import jax
import jax.numpy as jnp
from jax import lax
from jax.experimental import pallas as pl
from jax.experimental.pallas import tpu as pltpu
from jax.sharding import PartitionSpec as P


NOPE = 64
ROPE = 32
VALUE_DIM = 64
HEAD = NOPE + ROPE
LATENT = 256
REACH = 8
eps = 1e-06
theta = 10000.0
bf = jnp.bfloat16
f32 = jnp.float32

PAY = LATENT + ROPE + 16
ACC = VALUE_DIM + 16


def sp_of(z, y, c):
    return (z % 4) * 8 + (y % 4) * 2 + c


SITES = [(z, y, c) for z in range(4) for y in range(4) for c in range(2)]
SWAP = [(sp_of(z, y, c), sp_of(z, y, 1 - c)) for z, y, c in SITES]


def along(step, second):
    pairs = []
    for z, y, c in SITES:
        on_z = (c == 0) != second
        pairs.append((sp_of(z, y, c), sp_of(z + step, y, c) if on_z else sp_of(z, y + step, c)))
    return pairs


def ring(step):
    return [(i, (i + step) % 4) for i in range(4)]


def params(mib=56):
    return pltpu.CompilerParams(vmem_limit_bytes=mib * 2**20)


VM = pl.BlockSpec(memory_space=pltpu.VMEM)
SM = pl.BlockSpec(memory_space=pltpu.SMEM)


def gained(x, gain):
    return (x * gain).astype(bf)


def load_kernel(*refs, count):
    outs, sems = refs[-count - 1 : -1], refs[-1]
    copies = [pltpu.make_async_copy(refs[i], outs[i], sems.at[i]) for i in range(count)]
    for copy in copies:
        copy.start()
    for copy in copies:
        copy.wait()


def project_kernel(ids, x0, x1, x2, gain, wl, wr, wqd, wpi, square, lat, raw, query, pool):
    values, ns, ats = pieces_of(ids, (x0, x1, x2), gain)
    total = sum(jnp.sum(x * x, axis=-1, keepdims=True) for x in values)
    square[...] = jnp.broadcast_to(total, square.shape)
    lat[...] = summed(ns, wl, ats)
    raw[...] = sum(product(n, wr[:, pl.ds(at, 512)], True) for n, at in zip(ns, ats))
    query[...] = summed(ns, wqd, ats)
    pool[...] = summed(ns, wpi, ats)


def pieces_of(ids, xs, gain):
    ats = [pl.multiple_of(ids[k] * 512, 512) for k in range(len(xs))]
    values = [x[...].astype(f32) for x in xs]
    return values, [gained(x, gain[:, pl.ds(at, 512)]) for x, at in zip(values, ats)], ats


def all_pieces(ids, x0, x1, x2, xa, xb, gain):
    _, ns, ats = pieces_of(ids, (x0, x1, x2), gain)
    _, n, at = last_piece(ids, xa, xb, gain)
    return ns + [n], ats + [at]


def summed(ns, w, ats):
    return sum(product(n, rows_at(w, at), False) for n, at in zip(ns, ats))


def product(n, w, turned):
    if turned:
        return lax.dot_general(w, n, (((1,), (1,)), ((), ())), preferred_element_type=f32)
    return jnp.dot(n, w, preferred_element_type=f32)


def rows_at(w, at):
    return w[pl.ds(at, 512), :]


def last_piece(ids, xa, xb, gain):
    at = pl.multiple_of(ids[3] * 512, 512)
    x = jnp.concatenate([xa[...], xb[...]], axis=0).astype(f32)
    return x, gained(x, gain[:, pl.ds(at, 512)]), at


def front_kernel(ids, xa, xb, gain, wl, wr, square, lat0, raw0, gains, cos, sin, pay, scale_out):
    x, n, at = last_piece(ids, xa, xb, gain)
    lgain, kgain = gains[:LATENT], gains[LATENT + NOPE : LATENT + HEAD]
    total = square[...] + jnp.broadcast_to(jnp.sum(x * x, axis=-1, keepdims=True), square.shape)
    scale = lax.rsqrt(total * (1.0 / 2048) + eps)
    scale_out[...] = scale
    lat = lat0[...] + product(n, rows_at(wl, at), False)
    lat = jnp.transpose(lat * scale[:, :1]).astype(bf).astype(f32)
    lat = lat * lax.rsqrt(jnp.mean(lat * lat, axis=0, keepdims=True) + eps) * lgain
    pay[:LATENT, :] = lat.astype(bf)
    raw = raw0[...] + product(n, wr[:, pl.ds(at, 512)], True)
    raw = (raw * jnp.transpose(scale)[:1]).astype(bf).astype(f32)
    total = jnp.sum(raw * raw, axis=0, keepdims=True)
    k = raw * kgain
    first, second = k[:16], k[16:]
    pay[LATENT : LATENT + 16, :] = (first * cos[...] - second * sin[...]).astype(bf)
    pay[LATENT + 16 : LATENT + 32, :] = (first * sin[...] + second * cos[...]).astype(bf)
    pay[LATENT + 32 :, :] = jnp.broadcast_to(total, (16, total.shape[1])).astype(bf)


def query_kernel(ids, xa, xb, gain, wqd, wpi, scale, query0, pool0, qgain, wqu, gains, cos, sin, q, pool_in, outer):
    _, n, at = last_piece(ids, xa, xb, gain)
    hgain = gains[LATENT + HEAD : LATENT + 2 * HEAD]
    s = scale[:, :1]
    pooled = (pool0[...] + product(n, rows_at(wpi, at), False)) * s
    pool_in[...] = pooled.astype(bf)
    head, end = pooled[:REACH], pooled[pooled.shape[0] - REACH :]
    on_first = ids[8] % 2 == 0
    inner = jnp.concatenate([jnp.where(on_first, end, head)] * 2, axis=0).astype(bf)
    q[q.shape[0] - 16 :, :] = jnp.concatenate([inner, inner[:, :128]], axis=1)
    outer[...] = jnp.where(on_first, head, end).astype(bf)
    lat = (query0[...] + product(n, rows_at(wqd, at), False)) * s
    lat = lat.astype(bf).astype(f32)
    lat = lat * lax.rsqrt(jnp.mean(lat * lat, axis=-1, keepdims=True) + eps) * qgain[...]
    raw = jnp.dot(lat.astype(bf), wqu[...], preferred_element_type=f32)
    raw = jnp.transpose(raw).astype(bf).astype(f32)
    for h in range(raw.shape[0] // HEAD):
        v = raw[h * HEAD : (h + 1) * HEAD]
        v = v * lax.rsqrt(jnp.mean(v * v, axis=0, keepdims=True) + eps) * hgain
        v = v * (HEAD**-0.5 / math.log(2.0))
        first, second = v[NOPE : NOPE + 16], v[NOPE + 16 :]
        base = h * HEAD
        q[base : base + NOPE, :] = v[:NOPE].astype(bf)
        q[base + NOPE : base + NOPE + 16, :] = (first * cos[...] - second * sin[...]).astype(bf)
        q[base + NOPE + 16 : base + HEAD, :] = (first * sin[...] + second * cos[...]).astype(bf)


def gate_kernel(ids, x0, x1, x2, xa, xb, gain, wa, wp, scale, gate_a, gate_p):
    ns, ats = all_pieces(ids, x0, x1, x2, xa, xb, gain)
    s = scale[:, :1]
    gate_a[...] = jax.nn.sigmoid(summed(ns, wa, ats) * s)
    gate_p[...] = jax.nn.sigmoid(summed(ns, wp, ats) * s)


def join_kernel(a, b, c, d, out):
    width = a.shape[1]
    for i, x in enumerate((a, b, c, d)):
        out[:, i * width : (i + 1) * width] = x[...]


def chosen(ids, packs, kind):
    mine, other = packs
    take_mine = ids[8] % 2 == kind
    return jnp.where(take_mine, mine[:256, :], other[:256, :])


def pool_merge_kernel(ids, pool, attn, own, f1, f2, f3, s1, s2, s3, gate_a, gate_p, out, attn_w):
    total = jnp.dot(pool[...], own[256:, :], preferred_element_type=f32)
    for k, (f, s) in enumerate(((f1, s1), (f2, s2), (f3, s3))):
        p = jnp.concatenate([f[256:, :256], f[256:, 256:]], axis=0)
        total = total + jnp.dot(p, chosen(ids, (f, s), 1), preferred_element_type=f32)
        attn_w[k * 256 : (k + 1) * 256, :] = chosen(ids, (f, s), 0)
    first = lax.dot_general(attn[...], own[:256, :], (((0,), (0,)), ((), ())), preferred_element_type=f32)
    out[...] = gate_p[...] * total + gate_a[...] * first


def pack_kernel(ids, inner, x, outer, mix, scale, wa, wp, pool, own, s1, s2, s3, padded, sum2, sum4, sum8):
    rows = x.shape[0]
    half, length = ids[9], ids[10]
    on_first = ids[8] % 2 == 0
    inner = inner[inner.shape[0] - 16 :, :256][:REACH].astype(f32)
    outer = outer[...].astype(f32)
    padded[0:REACH, :] = jnp.where(on_first, outer, inner)
    padded[REACH : REACH + rows, :] = x[...].astype(f32)
    padded[REACH + rows :, :] = jnp.where(on_first, inner, outer)
    n = rows + 2 * REACH
    sum2[: n - 1, :] = padded[: n - 1, :] + padded[1:n, :]
    sum4[: n - 3, :] = sum2[: n - 3, :] + sum2[2 : n - 1, :]
    sum8[: n - 7, :] = sum4[: n - 7, :] + sum4[4 : n - 3, :]
    total = sum8[:rows, :] + sum8[REACH : REACH + rows, :]
    total = jnp.where(half == 4, sum8[4 : 4 + rows, :], total)
    total = jnp.where(half == 2, sum4[6 : 6 + rows, :], total)
    total = jnp.where(half == 1, sum2[7 : 7 + rows, :], total)
    at = ids[8] * rows + lax.broadcasted_iota(jnp.int32, (rows, 1), 0)
    count = (jnp.clip(at + half, 0, length) - jnp.clip(at - half, 0, length)).astype(f32)
    mixed = (total / count - padded[REACH : REACH + rows, :]).astype(bf)
    out = (jnp.dot(mixed, mix[...], preferred_element_type=f32) * scale[...]).astype(bf)
    pool[...] = out
    at = pl.multiple_of(ids[4] * 512, 512)
    own[:256, :] = wa[:, pl.ds(at, 512)]
    own[256:, :] = wp[:, pl.ds(at, 512)]
    for d, s in ((1, s1), (2, s2), (3, s3)):
        at = pl.multiple_of(ids[4 + d] * 512, 512)
        s[:256, :] = jnp.where(on_first, wa[:, pl.ds(at, 512)], wp[:, pl.ds(at, 512)])
        s[256:, :256] = out[: rows // 2]
        s[256:, 256:] = out[rows // 2 :]


def attend_kernel(*refs, pieces, seeded):
    q0, q1, up, gains = refs[:4]
    refs = refs[4:]
    gain = gains[LATENT : LATENT + NOPE]
    n_in = sum(len(p) for p in pieces)
    blocks = refs[:n_in]
    refs = refs[n_in:]
    seeds, outs = (refs[:2], refs[2:]) if seeded else ((), refs)
    heads = q0.shape[0] // HEAD
    half = q0.shape[1]
    at = 0
    for number, piece in enumerate(pieces):
        parts = [blocks[at + i] for i in range(len(piece))]
        at += len(piece)
        whole = parts[0][...] if len(parts) == 1 else jnp.concatenate([p[...] for p in parts], axis=0)
        keys = whole.shape[1]
        latent = whole[:LATENT]
        rope = whole[LATENT : LATENT + ROPE].astype(f32)
        square = whole[LATENT + ROPE :].astype(f32)[0:1]
        expanded = lax.dot_general(up[...], latent, (((0,), (0,)), ((), ())), preferred_element_type=f32)
        row = lax.broadcasted_iota(jnp.int32, (16, keys), 0)
        ones = jnp.where(row == 0, 1.0, 0.0).astype(bf)
        for h in range(heads):
            k = expanded[h * 128 : h * 128 + NOPE]
            scale = lax.rsqrt((jnp.sum(k * k, axis=0, keepdims=True) + square) * (1.0 / HEAD) + eps)
            key = jnp.concatenate([(k * gain * scale).astype(bf), (rope * scale).astype(bf)], axis=0)
            query = jnp.concatenate([q[h * HEAD : (h + 1) * HEAD, :] for q in (q0, q1)], axis=1)
            scores = lax.dot_general(key, query, (((0,), (0,)), ((), ())), preferred_element_type=f32)
            weights = jnp.exp2(scores).astype(bf)
            v = jnp.concatenate([expanded[h * 128 + NOPE : (h + 1) * 128].astype(bf), ones], axis=0)
            add = jnp.dot(v, weights, preferred_element_type=f32)
            for i in range(2):
                part = add[:, i * half : (i + 1) * half]
                if number > 0:
                    outs[i][h] += part
                elif seeded:
                    outs[i][h] = (seeds[i][h] + part).astype(outs[i].dtype)
                else:
                    outs[i][h] = part


def attend(q0, q1, up, gains, pieces, seeds, sent_type=f32):
    heads, half = q0.shape[0] // HEAD, q0.shape[1]
    shape = jax.ShapeDtypeStruct((heads, ACC, half), f32)
    arrays = [a for p in pieces for a in p]
    keys = sum(p[0].shape[1] for p in pieces)
    kernel = functools.partial(
        attend_kernel, pieces=[[None] * len(p) for p in pieces], seeded=seeds is not None
    )
    return call(
        kernel,
        None,
        [q0, q1, up, gains, *[resident(a) for a in (*arrays, *(seeds or ()))]],
        [kept(shape), kept(jax.ShapeDtypeStruct(shape.shape, sent_type))],
        keys * heads * 2 * half * 2 * 512,
        mib=28,
        transcendentals=keys * heads * 2 * half,
    )


def finish_kernel(mine, other, out):
    for h in range(mine.shape[0]):
        both = mine[h] + other[h].astype(f32)
        out[h * VALUE_DIM : (h + 1) * VALUE_DIM, :] = (
            both[:VALUE_DIM] / both[VALUE_DIM : VALUE_DIM + 1]
        ).astype(bf)


def merge_kernel(a1, a2, a3, w, gate, rest, out):
    a = jnp.concatenate([a1[...], a2[...], a3[...]], axis=0)
    total = lax.dot_general(a, w[...], (((0,), (0,)), ((), ())), preferred_element_type=f32)
    out[...] = (gate[...] * total + rest[...]).astype(bf)


def resident(x):
    return pltpu.with_memory_space_constraint(x, pltpu.VMEM)


def kept(s):
    return pltpu.VMEM(s.shape, s.dtype)


def call(kernel, ids, ins, shapes, flops, scratch=(), mib=16, transcendentals=0, apart=()):
    first = [] if ids is None else [ids]
    ins = [pltpu.with_memory_space_constraint(x, pltpu.HBM) if i in apart else x for i, x in enumerate(ins)]
    return pl.pallas_call(
        kernel,
        in_specs=[SM] * len(first)
        + [pl.BlockSpec(memory_space=pltpu.HBM) if i in apart else VM for i in range(len(ins))],
        out_specs=jax.tree.map(lambda _: VM, shapes),
        out_shape=shapes,
        scratch_shapes=scratch,
        compiler_params=params(mib),
        cost_estimate=pl.CostEstimate(flops=flops, transcendentals=transcendentals, bytes_accessed=2**20),
    )(*first, *ins)


def whole(
    tokens,
    norm_gain,
    w_query_down,
    query_gain,
    w_query_up,
    w_latent_down,
    latent_gain,
    w_rotary_key,
    w_latent_up,
    query_head_gain,
    key_head_gain,
    w_pool_in,
    w_pool_mix,
    pool_scale,
    w_attn_out,
    w_pool_out,
    w_gate_attn,
    w_gate_pool,
):
    S = jax.ShapeDtypeStruct
    rows = tokens.shape[0]
    heads = w_query_up.shape[1] // HEAD
    length = rows * lax.axis_size("sp")
    here = lax.axis_index("sp")
    t = lax.axis_index("tp")

    x1 = lax.ppermute(tokens, "tp", ring(1))
    x2 = lax.ppermute(tokens, "tp", ring(-1))
    xa = lax.ppermute(x1[: rows // 2], "tp", ring(1))
    xb = lax.ppermute(x2[rows // 2 :], "tp", ring(-1))

    half = ROPE // 2
    freqs = theta ** (-jnp.arange(half, dtype=f32) / half)
    positions = (here * rows + jnp.arange(rows, dtype=jnp.int32)).astype(f32)
    angles = freqs[:, None] * positions[None, :]
    cos, sin = jnp.cos(angles), jnp.sin(angles)
    ids = jnp.concatenate(
        [
            (t + jnp.array([0, 3, 1, 2, 0, 1, 2, 3], jnp.int32)) & 3,
            jnp.stack([here, jnp.left_shift(1, t), jnp.int32(length)]).astype(jnp.int32),
        ]
    )
    gains = jnp.concatenate([latent_gain, key_head_gain, query_head_gain])[:, None]
    gain = norm_gain[None, :]
    wr = w_rotary_key.T

    wanted = [w_latent_down, wr, w_query_down, w_pool_in, w_query_up, gain, tokens, gains, cos, sin, query_gain[None, :]]
    wl, wr, wqd, wpi, wqu, gain, x0, near_gains, cos, sin, qgain = [
        resident(x)
        for x in call(
            functools.partial(load_kernel, count=11),
            None, [*wanted, ids], [kept(S(x.shape, x.dtype)) for x in wanted], 4 * 10**8,
            [pltpu.SemaphoreType.DMA((11,))], apart=range(12),
        )
    ]
    square, lat0, raw0, query0, pool0 = [
        resident(x)
        for x in call(
            project_kernel,
            ids, [x0, resident(x1), resident(x2), gain, wl, wr, wqd, wpi],
            [kept(S(s, f32)) for s in ((rows, 128), (rows, LATENT), (ROPE, rows), (rows, 512), (rows, 256))],
            16 * 10**8,
        )
    ]
    pay, scale = call(
        front_kernel,
        ids,
        [resident(xa), resident(xb), gain, wl, wr, square, lat0, raw0, near_gains, cos, sin],
        [kept(S((PAY, rows), bf)), kept(S((rows, 128), f32))],
        3 * 10**8,
    )
    pieces = [tokens, x1, x2, xa, xb]

    a1 = lax.ppermute(pay, "sp", along(1, False))
    a2 = lax.ppermute(pay, "sp", along(-1, False))
    a3 = lax.ppermute(pay, "sp", along(2, False))

    q, pool_in, outer = call(
        query_kernel,
        ids,
        [resident(xa), resident(xb), gain, wqd, wpi, resident(scale), query0, pool0, qgain,
         wqu, near_gains, cos, sin],
        [S((heads * HEAD + 16, rows), bf), S((rows, 256), bf), S((REACH, 256), bf)],
        10**9,
    )
    q_other = lax.ppermute(q, "sp", SWAP)
    count = lax.axis_size("sp")
    outer = lax.ppermute(outer, "sp", [(i, i - 1 + 2 * (i % 2)) for i in range(1, count - 1)])

    def attend_on(pieces, seeds, name):
        return attend(q, q_other, w_latent_up, gains, pieces, seeds, bf if name == "attend_far" else f32)

    line = call(join_kernel, None, [resident(x) for x in (pay, a1, a2, a3)], kept(S((PAY, 4 * rows), bf)), 10**7)
    b1 = lax.ppermute(line, "sp", along(1, True))
    b2 = lax.ppermute(line, "sp", along(-1, True))
    cut = PAY // 2
    b3 = lax.ppermute(b1[:cut], "sp", along(1, True))
    b4 = lax.ppermute(b2[cut:], "sp", along(-1, True))

    pool, own_w, *packs = call(
        pack_kernel,
        ids,
        [q_other, pool_in, outer, w_pool_mix[0], pool_scale[None, :], w_attn_out, w_pool_out],
        [S((rows, 256), bf), S((512, 512), bf)] + [S((448, 512), bf)] * 3,
        10**8,
        [pltpu.VMEM((rows + 2 * REACH, 256), f32)] * 4,
    )
    packs = [lax.ppermute(packs[d - 1], "tp", ring(d)) for d in (1, 2, 3)]
    swapped = [lax.ppermute(p, "sp", SWAP) for p in packs]
    weights = [own_w, *packs, *swapped]

    acc = attend_on([[line]], None, "attend_line")
    acc = attend_on([[b1], [b2]], acc, "attend_near")
    acc = attend_on([[b3, b4]], acc, "attend_far")

    gate_attn, gate_pool = call(
        gate_kernel,
        ids,
        [*pieces, norm_gain[None, :], w_gate_attn, w_gate_pool, scale],
        [kept(S((rows, 512), f32))] * 2,
        5 * 10**8,
    )
    other = lax.ppermute(acc[1], "sp", SWAP)
    attn = call(finish_kernel, None, [resident(acc[0]), resident(other)], kept(S((heads * VALUE_DIM, rows), bf)), 10**7)
    attns = [attn] + [lax.ppermute(attn, "tp", ring(d)) for d in (1, 2, 3)]
    rest, attn_w = call(
        pool_merge_kernel, ids, [pool, attn, *weights, resident(gate_attn), resident(gate_pool)],
        [kept(S((rows, 512), f32)), kept(S((768, 512), bf))], 10**9,
    )
    return call(
        merge_kernel,
        None,
        [*[resident(a) for a in attns[1:]], resident(attn_w), resident(gate_attn), resident(rest)],
        S((rows, 512), bf), 10**9,
    )


def solution(mesh):
    placed = (
        P("sp", "tp"),
        P(),
        P(),
        P(),
        P(None, "tp"),
        P(),
        P(),
        P(),
        P(None, "tp"),
        P(),
        P(),
        P(None, "tp"),
        P("tp", None, None),
        P("tp"),
        P("tp", None),
        P("tp", None),
        P(None, "tp"),
        P(None, "tp"),
    )
    return jax.shard_map(whole, mesh=mesh, in_specs=placed, out_specs=P("sp", "tp"), check_vma=False)
```

```python
import functools
import math

import jax
import jax.numpy as jnp
from jax import lax
from jax.experimental import pallas as pl
from jax.experimental.pallas import tpu as pltpu
from jax.sharding import PartitionSpec as P


NOPE = 64
ROPE = 32
VALUE_DIM = 64
HEAD = NOPE + ROPE
LATENT = 256
REACH = 8
eps = 1e-06
theta = 10000.0
bf = jnp.bfloat16
f32 = jnp.float32

PAY = LATENT + ROPE + 16
ACC = VALUE_DIM + 16


def sp_of(z, y, c):
    return (z % 4) * 8 + (y % 4) * 2 + c


SITES = [(z, y, c) for z in range(4) for y in range(4) for c in range(2)]
SWAP = [(sp_of(z, y, c), sp_of(z, y, 1 - c)) for z, y, c in SITES]


def along(step, second):
    pairs = []
    for z, y, c in SITES:
        on_z = (c == 0) != second
        pairs.append((sp_of(z, y, c), sp_of(z + step, y, c) if on_z else sp_of(z, y + step, c)))
    return pairs


def ring(step):
    return [(i, (i + step) % 4) for i in range(4)]


def params(mib=56):
    return pltpu.CompilerParams(vmem_limit_bytes=mib * 2**20)


VM = pl.BlockSpec(memory_space=pltpu.VMEM)
SM = pl.BlockSpec(memory_space=pltpu.SMEM)


def gained(x, gain):
    return (x * gain).astype(bf)


def load_kernel(*refs, count):
    outs, gains, sems = refs[-count - 2 : -2], refs[-2], refs[-1]
    copies = [pltpu.make_async_copy(refs[i], outs[i], sems.at[i]) for i in range(count)]
    for copy in copies:
        copy.start()
    row = refs[count][...]
    gains[...] = jnp.transpose(jnp.broadcast_to(row, (8, row.shape[1])))[:, :1]
    for copy in copies:
        copy.wait()


def project_kernel(ids, x0, x1a, x1b, x2a, x2b, gain, wl, wr, wqd, wpi, square, lat, raw, query, pool):
    values, ns, ats = pieces_of(ids, (x0, (x1a, x1b), (x2a, x2b)), gain)
    total = sum(jnp.sum(x * x, axis=-1, keepdims=True) for x in values)
    square[...] = jnp.broadcast_to(total, square.shape)
    lat[...] = summed(ns, wl, ats)
    raw[...] = sum(product(n, wr[:, pl.ds(at, 512)], True) for n, at in zip(ns, ats))
    query[...] = summed(ns, wqd, ats)
    pool[...] = summed(ns, wpi, ats)


def stacked(x):
    return jnp.concatenate([p[...] for p in x], axis=0) if isinstance(x, tuple) else x[...]


def pieces_of(ids, xs, gain):
    ats = [pl.multiple_of(ids[k] * 512, 512) for k in range(len(xs))]
    values = [stacked(x).astype(f32) for x in xs]
    return values, [gained(x, gain[:, pl.ds(at, 512)]) for x, at in zip(values, ats)], ats


def all_pieces(ids, x0, x1a, x1b, x2a, x2b, xa, xb, gain):
    _, ns, ats = pieces_of(ids, (x0, (x1a, x1b), (x2a, x2b)), gain)
    _, n, at = last_piece(ids, xa, xb, gain)
    return ns + [n], ats + [at]


def summed(ns, w, ats):
    return sum(product(n, rows_at(w, at), False) for n, at in zip(ns, ats))


def product(n, w, turned):
    if turned:
        return lax.dot_general(w, n, (((1,), (1,)), ((), ())), preferred_element_type=f32)
    return jnp.dot(n, w, preferred_element_type=f32)


def rows_at(w, at):
    return w[pl.ds(at, 512), :]


def last_piece(ids, xa, xb, gain):
    at = pl.multiple_of(ids[3] * 512, 512)
    x = jnp.concatenate([xa[...], xb[...]], axis=0).astype(f32)
    return x, gained(x, gain[:, pl.ds(at, 512)]), at


def front_kernel(ids, xa, xb, gain, wl, wr, square, lat0, raw0, gains, cos, sin, pay, scale_out):
    x, n, at = last_piece(ids, xa, xb, gain)
    lgain, kgain = gains[:LATENT], gains[LATENT + NOPE : LATENT + HEAD]
    total = square[...] + jnp.broadcast_to(jnp.sum(x * x, axis=-1, keepdims=True), square.shape)
    scale = lax.rsqrt(total * (1.0 / 2048) + eps)
    scale_out[...] = scale
    lat = lat0[...] + product(n, rows_at(wl, at), False)
    lat = jnp.transpose(lat * scale[:, :1]).astype(bf).astype(f32)
    lat = lat * lax.rsqrt(jnp.mean(lat * lat, axis=0, keepdims=True) + eps) * lgain
    pay[:LATENT, :] = lat.astype(bf)
    raw = raw0[...] + product(n, wr[:, pl.ds(at, 512)], True)
    raw = (raw * jnp.transpose(scale)[:1]).astype(bf).astype(f32)
    total = jnp.sum(raw * raw, axis=0, keepdims=True)
    k = raw * kgain
    first, second = k[:16], k[16:]
    pay[LATENT : LATENT + 16, :] = (first * cos[...] - second * sin[...]).astype(bf)
    pay[LATENT + 16 : LATENT + 32, :] = (first * sin[...] + second * cos[...]).astype(bf)
    pay[LATENT + 32 :, :] = jnp.broadcast_to(total, (16, total.shape[1])).astype(bf)


def query_kernel(ids, xa, xb, gain, wqd, wpi, scale, query0, pool0, qgain, wqu, gains, cos, sin, q, pool_in, outer):
    _, n, at = last_piece(ids, xa, xb, gain)
    hgain = gains[LATENT + HEAD : LATENT + 2 * HEAD]
    s = scale[:, :1]
    pooled = (pool0[...] + product(n, rows_at(wpi, at), False)) * s
    pool_in[...] = pooled.astype(bf)
    head, end = pooled[:REACH], pooled[pooled.shape[0] - REACH :]
    on_first = ids[8] % 2 == 0
    inner = jnp.concatenate([jnp.where(on_first, end, head)] * 2, axis=0).astype(bf)
    q[q.shape[0] - 16 :, :] = jnp.concatenate([inner, inner[:, :128]], axis=1)
    outer[...] = jnp.where(on_first, head, end).astype(bf)
    lat = (query0[...] + product(n, rows_at(wqd, at), False)) * s
    lat = lat.astype(bf).astype(f32)
    lat = lat * lax.rsqrt(jnp.mean(lat * lat, axis=-1, keepdims=True) + eps) * qgain[...]
    raw = jnp.dot(lat.astype(bf), wqu[...], preferred_element_type=f32)
    raw = jnp.transpose(raw).astype(bf).astype(f32)
    for h in range(raw.shape[0] // HEAD):
        v = raw[h * HEAD : (h + 1) * HEAD]
        v = v * lax.rsqrt(jnp.mean(v * v, axis=0, keepdims=True) + eps) * hgain
        v = v * (HEAD**-0.5 / math.log(2.0))
        first, second = v[NOPE : NOPE + 16], v[NOPE + 16 :]
        base = h * HEAD
        q[base : base + NOPE, :] = v[:NOPE].astype(bf)
        q[base + NOPE : base + NOPE + 16, :] = (first * cos[...] - second * sin[...]).astype(bf)
        q[base + NOPE + 16 : base + HEAD, :] = (first * sin[...] + second * cos[...]).astype(bf)


def gate_kernel(ids, x0, x1a, x1b, x2a, x2b, xa, xb, gain, wa, wp, scale, gate_a, gate_p):
    ns, ats = all_pieces(ids, x0, x1a, x1b, x2a, x2b, xa, xb, gain)
    s = scale[:, :1]
    gate_a[...] = jax.nn.sigmoid(summed(ns, wa, ats) * s)
    gate_p[...] = jax.nn.sigmoid(summed(ns, wp, ats) * s)


def join_kernel(a, b, c, d, out):
    width = a.shape[1]
    for i, x in enumerate((a, b, c, d)):
        out[:, i * width : (i + 1) * width] = x[...]


def chosen(ids, packs, kind):
    mine, other = packs
    take_mine = ids[8] % 2 == kind
    return jnp.where(take_mine, mine[:256, :], other[:256, :])


def pool_merge_kernel(ids, pool, attn, own, f1, f2, f3, s1, s2, s3, gate_a, gate_p, out, attn_w):
    total = jnp.dot(pool[...], own[256:, :], preferred_element_type=f32)
    for k, (f, s) in enumerate(((f1, s1), (f2, s2), (f3, s3))):
        p = jnp.concatenate([f[256:, :256], f[256:, 256:]], axis=0)
        total = total + jnp.dot(p, chosen(ids, (f, s), 1), preferred_element_type=f32)
        attn_w[k * 256 : (k + 1) * 256, :] = chosen(ids, (f, s), 0)
    first = lax.dot_general(attn[...], own[:256, :], (((0,), (0,)), ((), ())), preferred_element_type=f32)
    out[...] = gate_p[...] * total + gate_a[...] * first


def pack_kernel(ids, inner, x, outer, mix, scale, wa, wp, pool, own, s1, s2, s3, padded, sum2, sum4, sum8):
    rows = x.shape[0]
    half, length = ids[9], ids[10]
    on_first = ids[8] % 2 == 0
    inner = inner[inner.shape[0] - 16 :, :256][:REACH].astype(f32)
    outer = outer[...].astype(f32)
    padded[0:REACH, :] = jnp.where(on_first, outer, inner)
    padded[REACH : REACH + rows, :] = x[...].astype(f32)
    padded[REACH + rows :, :] = jnp.where(on_first, inner, outer)
    n = rows + 2 * REACH
    sum2[: n - 1, :] = padded[: n - 1, :] + padded[1:n, :]
    sum4[: n - 3, :] = sum2[: n - 3, :] + sum2[2 : n - 1, :]
    sum8[: n - 7, :] = sum4[: n - 7, :] + sum4[4 : n - 3, :]
    total = sum8[:rows, :] + sum8[REACH : REACH + rows, :]
    total = jnp.where(half == 4, sum8[4 : 4 + rows, :], total)
    total = jnp.where(half == 2, sum4[6 : 6 + rows, :], total)
    total = jnp.where(half == 1, sum2[7 : 7 + rows, :], total)
    at = ids[8] * rows + lax.broadcasted_iota(jnp.int32, (rows, 1), 0)
    count = (jnp.clip(at + half, 0, length) - jnp.clip(at - half, 0, length)).astype(f32)
    mixed = (total / count - padded[REACH : REACH + rows, :]).astype(bf)
    out = (jnp.dot(mixed, mix[...], preferred_element_type=f32) * scale[...]).astype(bf)
    pool[...] = out
    at = pl.multiple_of(ids[4] * 512, 512)
    own[:256, :] = wa[:, pl.ds(at, 512)]
    own[256:, :] = wp[:, pl.ds(at, 512)]
    for d, s in ((1, s1), (2, s2), (3, s3)):
        at = pl.multiple_of(ids[4 + d] * 512, 512)
        s[:256, :] = jnp.where(on_first, wa[:, pl.ds(at, 512)], wp[:, pl.ds(at, 512)])
        s[256:, :256] = out[: rows // 2]
        s[256:, 256:] = out[rows // 2 :]


def attend_kernel(*refs, pieces, seeded):
    q0, q1, up, gains = refs[:4]
    refs = refs[4:]
    gain = gains[LATENT : LATENT + NOPE]
    n_in = sum(len(p) for p in pieces)
    blocks = refs[:n_in]
    refs = refs[n_in:]
    seeds, outs = (refs[:2], refs[2:]) if seeded else ((), refs)
    heads = q0.shape[0] // HEAD
    half = q0.shape[1]
    at = 0
    for number, piece in enumerate(pieces):
        parts = [blocks[at + i] for i in range(len(piece))]
        at += len(piece)
        whole = parts[0][...] if len(parts) == 1 else jnp.concatenate([p[...] for p in parts], axis=0)
        keys = whole.shape[1]
        latent = whole[:LATENT]
        rope = whole[LATENT : LATENT + ROPE].astype(f32)
        square = whole[LATENT + ROPE :].astype(f32)[0:1]
        expanded = lax.dot_general(up[...], latent, (((0,), (0,)), ((), ())), preferred_element_type=f32)
        row = lax.broadcasted_iota(jnp.int32, (16, keys), 0)
        ones = jnp.where(row == 0, 1.0, 0.0).astype(bf)
        for h in range(heads):
            k = expanded[h * 128 : h * 128 + NOPE]
            scale = lax.rsqrt((jnp.sum(k * k, axis=0, keepdims=True) + square) * (1.0 / HEAD) + eps)
            key = jnp.concatenate([(k * gain * scale).astype(bf), (rope * scale).astype(bf)], axis=0)
            query = jnp.concatenate([q[h * HEAD : (h + 1) * HEAD, :] for q in (q0, q1)], axis=1)
            scores = lax.dot_general(key, query, (((0,), (0,)), ((), ())), preferred_element_type=f32)
            weights = jnp.exp2(scores).astype(bf)
            v = jnp.concatenate([expanded[h * 128 + NOPE : (h + 1) * 128].astype(bf), ones], axis=0)
            add = jnp.dot(v, weights, preferred_element_type=f32)
            for i in range(2):
                part = add[:, i * half : (i + 1) * half]
                if number > 0:
                    outs[i][h] += part
                elif seeded:
                    outs[i][h] = (seeds[i][h] + part).astype(outs[i].dtype)
                else:
                    outs[i][h] = part


def attend(q0, q1, up, gains, pieces, seeds, sent_type=f32):
    heads, half = q0.shape[0] // HEAD, q0.shape[1]
    shape = jax.ShapeDtypeStruct((heads, ACC, half), f32)
    arrays = [a for p in pieces for a in p]
    keys = sum(p[0].shape[1] for p in pieces)
    kernel = functools.partial(
        attend_kernel, pieces=[[None] * len(p) for p in pieces], seeded=seeds is not None
    )
    return call(
        kernel,
        None,
        [q0, q1, up, gains, *[resident(a) for a in (*arrays, *(seeds or ()))]],
        [kept(shape), kept(jax.ShapeDtypeStruct(shape.shape, sent_type))],
        keys * heads * 2 * half * 2 * 512,
        mib=28,
        transcendentals=keys * heads * 2 * half,
    )


def finish_kernel(mine, other, out):
    for h in range(mine.shape[0]):
        both = mine[h] + other[h].astype(f32)
        out[h * VALUE_DIM : (h + 1) * VALUE_DIM, :] = (
            both[:VALUE_DIM] / both[VALUE_DIM : VALUE_DIM + 1]
        ).astype(bf)


def merge_kernel(a1, a2, a3, w, gate, rest, out):
    a = jnp.concatenate([a1[...], a2[...], a3[...]], axis=0)
    total = lax.dot_general(a, w[...], (((0,), (0,)), ((), ())), preferred_element_type=f32)
    out[...] = (gate[...] * total + rest[...]).astype(bf)


def resident(x):
    return pltpu.with_memory_space_constraint(x, pltpu.VMEM)


def kept(s):
    return pltpu.VMEM(s.shape, s.dtype)


def call(kernel, ids, ins, shapes, flops, scratch=(), mib=16, transcendentals=0, apart=()):
    first = [] if ids is None else [ids]
    ins = [pltpu.with_memory_space_constraint(x, pltpu.HBM) if i in apart else x for i, x in enumerate(ins)]
    return pl.pallas_call(
        kernel,
        in_specs=[SM] * len(first)
        + [pl.BlockSpec(memory_space=pltpu.HBM) if i in apart else VM for i in range(len(ins))],
        out_specs=jax.tree.map(lambda _: VM, shapes),
        out_shape=shapes,
        scratch_shapes=scratch,
        compiler_params=params(mib),
        cost_estimate=pl.CostEstimate(flops=flops, transcendentals=transcendentals, bytes_accessed=2**20),
    )(*first, *ins)


def whole(
    tokens,
    norm_gain,
    w_query_down,
    query_gain,
    w_query_up,
    w_latent_down,
    latent_gain,
    w_rotary_key,
    w_latent_up,
    query_head_gain,
    key_head_gain,
    w_pool_in,
    w_pool_mix,
    pool_scale,
    w_attn_out,
    w_pool_out,
    w_gate_attn,
    w_gate_pool,
):
    S = jax.ShapeDtypeStruct
    rows = tokens.shape[0]
    heads = w_query_up.shape[1] // HEAD
    length = rows * lax.axis_size("sp")
    here = lax.axis_index("sp")
    t = lax.axis_index("tp")

    top, bottom = tokens[: rows // 2], tokens[rows // 2 :]
    x1a = lax.ppermute(top, "tp", ring(1))
    x2b = lax.ppermute(bottom, "tp", ring(-1))
    x1b = lax.ppermute(bottom, "tp", ring(1))
    x2a = lax.ppermute(top, "tp", ring(-1))
    xa = lax.ppermute(x1a, "tp", ring(1))
    xb = lax.ppermute(x2b, "tp", ring(-1))

    half = ROPE // 2
    freqs = theta ** (-jnp.arange(half, dtype=f32) / half)
    positions = (here * rows + jnp.arange(rows, dtype=jnp.int32)).astype(f32)
    angles = freqs[:, None] * positions[None, :]
    cos, sin = jnp.cos(angles), jnp.sin(angles)
    fixed = jnp.array([0, 3, 1, 2, 0, 1, 2, 3, 0, 0, length], jnp.int32)
    slot = jnp.arange(11, dtype=jnp.int32)
    ids = jnp.where(slot < 8, (fixed + t) & 3, fixed + (slot == 8) * here + (slot == 9) * jnp.left_shift(1, t))
    gains = jnp.concatenate([latent_gain, key_head_gain, query_head_gain, jnp.zeros((64,), f32)])[None, :]
    gain = norm_gain[None, :]
    wr = w_rotary_key.T

    wanted = [w_latent_down, wr, w_query_down, w_pool_in, w_query_up, gain, tokens, cos, sin, query_gain[None, :]]
    wl, wr, wqd, wpi, wqu, gain, x0, cos, sin, qgain, near_gains = [
        resident(x)
        for x in call(
            functools.partial(load_kernel, count=10),
            None, [*wanted, gains, ids], [kept(S(x.shape, x.dtype)) for x in wanted] + [kept(S((512, 1), f32))],
            4 * 10**8, [pltpu.SemaphoreType.DMA((10,))], apart=(*range(10), 11),
        )
    ]
    square, lat0, raw0, query0, pool0 = [
        resident(x)
        for x in call(
            project_kernel,
            ids, [x0, *[resident(x) for x in (x1a, x1b, x2a, x2b)], gain, wl, wr, wqd, wpi],
            [kept(S(s, f32)) for s in ((rows, 128), (rows, LATENT), (ROPE, rows), (rows, 512), (rows, 256))],
            16 * 10**8,
        )
    ]
    pay, scale = call(
        front_kernel,
        ids,
        [resident(xa), resident(xb), gain, wl, wr, square, lat0, raw0, near_gains, cos, sin],
        [kept(S((PAY, rows), bf)), kept(S((rows, 128), f32))],
        3 * 10**8,
    )
    pieces = [tokens, x1a, x1b, x2a, x2b, xa, xb]

    a1 = lax.ppermute(pay, "sp", along(1, False))
    a2 = lax.ppermute(pay, "sp", along(-1, False))
    a3 = lax.ppermute(pay, "sp", along(2, False))

    q, pool_in, outer = call(
        query_kernel,
        ids,
        [resident(xa), resident(xb), gain, wqd, wpi, resident(scale), query0, pool0, qgain,
         wqu, near_gains, cos, sin],
        [S((heads * HEAD + 16, rows), bf), S((rows, 256), bf), S((REACH, 256), bf)],
        10**9,
    )
    q_other = lax.ppermute(q, "sp", SWAP)
    count = lax.axis_size("sp")
    outer = lax.ppermute(outer, "sp", [(i, i - 1 + 2 * (i % 2)) for i in range(1, count - 1)])

    def attend_on(pieces, seeds, name):
        return attend(q, q_other, w_latent_up, near_gains, pieces, seeds, bf if name == "attend_far" else f32)

    line = call(join_kernel, None, [resident(x) for x in (pay, a1, a2, a3)], kept(S((PAY, 4 * rows), bf)), 10**7)
    b1 = lax.ppermute(line, "sp", along(1, True))
    b2 = lax.ppermute(line, "sp", along(-1, True))
    cut = PAY // 2
    b3 = lax.ppermute(b1[:cut], "sp", along(1, True))
    b4 = lax.ppermute(b2[cut:], "sp", along(-1, True))

    pool, own_w, *packs = call(
        pack_kernel,
        ids,
        [q_other, pool_in, outer, w_pool_mix[0], pool_scale[None, :], w_attn_out, w_pool_out],
        [S((rows, 256), bf), S((512, 512), bf)] + [S((448, 512), bf)] * 3,
        10**8,
        [pltpu.VMEM((rows + 2 * REACH, 256), f32)] * 4,
    )
    packs = [lax.ppermute(packs[d - 1], "tp", ring(d)) for d in (1, 2, 3)]
    swapped = [lax.ppermute(p, "sp", SWAP) for p in packs]
    weights = [own_w, *packs, *swapped]

    acc = attend_on([[line]], None, "attend_line")
    acc = attend_on([[b1], [b2]], acc, "attend_near")
    acc = attend_on([[b3, b4]], acc, "attend_far")

    gate_attn, gate_pool = call(
        gate_kernel,
        ids,
        [*pieces, norm_gain[None, :], w_gate_attn, w_gate_pool, scale],
        [kept(S((rows, 512), f32))] * 2,
        5 * 10**8,
    )
    other = lax.ppermute(acc[1], "sp", SWAP)
    attn = call(finish_kernel, None, [resident(acc[0]), resident(other)], kept(S((heads * VALUE_DIM, rows), bf)), 10**7)
    attns = [attn] + [lax.ppermute(attn, "tp", ring(d)) for d in (1, 2, 3)]
    rest, attn_w = call(
        pool_merge_kernel, ids, [pool, attn, *weights, resident(gate_attn), resident(gate_pool)],
        [kept(S((rows, 512), f32)), kept(S((768, 512), bf))], 10**9,
    )
    return call(
        merge_kernel,
        None,
        [*[resident(a) for a in attns[1:]], resident(attn_w), resident(gate_attn), resident(rest)],
        S((rows, 512), bf), 10**9,
    )


def solution(mesh):
    placed = (
        P("sp", "tp"),
        P(),
        P(),
        P(),
        P(None, "tp"),
        P(),
        P(),
        P(),
        P(None, "tp"),
        P(),
        P(),
        P(None, "tp"),
        P("tp", None, None),
        P("tp"),
        P("tp", None),
        P("tp", None),
        P(None, "tp"),
        P(None, "tp"),
    )
    return jax.shard_map(whole, mesh=mesh, in_specs=placed, out_specs=P("sp", "tp"), check_vma=False)
```

```python
import functools
import math

import jax
import jax.numpy as jnp
from jax import lax
from jax.experimental import pallas as pl
from jax.experimental.pallas import tpu as pltpu
from jax.sharding import PartitionSpec as P


NOPE = 64
ROPE = 32
VALUE_DIM = 64
HEAD = NOPE + ROPE
LATENT = 256
REACH = 8
eps = 1e-06
theta = 10000.0
bf = jnp.bfloat16
f32 = jnp.float32

PAY = LATENT + ROPE + 16
ACC = VALUE_DIM + 16


def sp_of(z, y, c):
    return (z % 4) * 8 + (y % 4) * 2 + c


SITES = [(z, y, c) for z in range(4) for y in range(4) for c in range(2)]
SWAP = [(sp_of(z, y, c), sp_of(z, y, 1 - c)) for z, y, c in SITES]


def along(step, second):
    pairs = []
    for z, y, c in SITES:
        on_z = (c == 0) != second
        pairs.append((sp_of(z, y, c), sp_of(z + step, y, c) if on_z else sp_of(z, y + step, c)))
    return pairs


def ring(step):
    return [(i, (i + step) % 4) for i in range(4)]


def params(mib=56):
    return pltpu.CompilerParams(vmem_limit_bytes=mib * 2**20)


VM = pl.BlockSpec(memory_space=pltpu.VMEM)
SM = pl.BlockSpec(memory_space=pltpu.SMEM)


def gained(x, gain):
    return (x * gain).astype(bf)


def load_kernel(*refs, count):
    outs, gains, sems = refs[-count - 2 : -2], refs[-2], refs[-1]
    copies = [pltpu.make_async_copy(refs[i], outs[i], sems.at[i]) for i in range(count)]
    for copy in copies:
        copy.start()
    row = refs[count][...]
    gains[...] = jnp.transpose(jnp.broadcast_to(row, (8, row.shape[1])))[:, :1]
    for copy in copies:
        copy.wait()


def project_kernel(ids, x0, x1a, x1b, x2a, x2b, gain, wl, wr, wqd, wpi, square, lat, raw, query, pool):
    values, ns, ats = pieces_of(ids, (x0, (x1a, x1b), (x2a, x2b)), gain)
    total = sum(jnp.sum(x * x, axis=-1, keepdims=True) for x in values)
    square[...] = jnp.broadcast_to(total, square.shape)
    lat[...] = summed(ns, wl, ats)
    raw[...] = sum(product(n, wr[:, pl.ds(at, 512)], True) for n, at in zip(ns, ats))
    query[...] = summed(ns, wqd, ats)
    pool[...] = summed(ns, wpi, ats)


def stacked(x):
    return jnp.concatenate([p[...] for p in x], axis=0) if isinstance(x, tuple) else x[...]


def pieces_of(ids, xs, gain):
    ats = [pl.multiple_of(ids[k] * 512, 512) for k in range(len(xs))]
    values = [stacked(x).astype(f32) for x in xs]
    return values, [gained(x, gain[:, pl.ds(at, 512)]) for x, at in zip(values, ats)], ats


def all_pieces(ids, x0, x1a, x1b, x2a, x2b, xa, xb, gain):
    _, ns, ats = pieces_of(ids, (x0, (x1a, x1b), (x2a, x2b)), gain)
    _, n, at = last_piece(ids, xa, xb, gain)
    return ns + [n], ats + [at]


def summed(ns, w, ats):
    return sum(product(n, rows_at(w, at), False) for n, at in zip(ns, ats))


def product(n, w, turned):
    if turned:
        return lax.dot_general(w, n, (((1,), (1,)), ((), ())), preferred_element_type=f32)
    return jnp.dot(n, w, preferred_element_type=f32)


def rows_at(w, at):
    return w[pl.ds(at, 512), :]


def last_piece(ids, xa, xb, gain):
    at = pl.multiple_of(ids[3] * 512, 512)
    x = jnp.concatenate([xa[...], xb[...]], axis=0).astype(f32)
    return x, gained(x, gain[:, pl.ds(at, 512)]), at


def front_kernel(ids, xa, xb, gain, wl, wr, square, lat0, raw0, gains, cos, sin, pay, scale_out):
    x, n, at = last_piece(ids, xa, xb, gain)
    lgain, kgain = gains[:LATENT], gains[LATENT + NOPE : LATENT + HEAD]
    total = square[...] + jnp.broadcast_to(jnp.sum(x * x, axis=-1, keepdims=True), square.shape)
    scale = lax.rsqrt(total * (1.0 / 2048) + eps)
    scale_out[...] = scale
    lat = lat0[...] + product(n, rows_at(wl, at), False)
    lat = jnp.transpose(lat * scale[:, :1]).astype(bf).astype(f32)
    lat = lat * lax.rsqrt(jnp.mean(lat * lat, axis=0, keepdims=True) + eps) * lgain
    pay[:LATENT, :] = lat.astype(bf)
    raw = raw0[...] + product(n, wr[:, pl.ds(at, 512)], True)
    raw = (raw * jnp.transpose(scale)[:1]).astype(bf).astype(f32)
    total = jnp.sum(raw * raw, axis=0, keepdims=True)
    k = raw * kgain
    first, second = k[:16], k[16:]
    pay[LATENT : LATENT + 16, :] = (first * cos[...] - second * sin[...]).astype(bf)
    pay[LATENT + 16 : LATENT + 32, :] = (first * sin[...] + second * cos[...]).astype(bf)
    pay[LATENT + 32 :, :] = jnp.broadcast_to(total, (16, total.shape[1])).astype(bf)


def query_kernel(ids, xa, xb, gain, wqd, wpi, scale, query0, pool0, qgain, wqu, gains, cos, sin, q, pool_in, outer):
    _, n, at = last_piece(ids, xa, xb, gain)
    hgain = gains[LATENT + HEAD : LATENT + 2 * HEAD]
    s = scale[:, :1]
    pooled = (pool0[...] + product(n, rows_at(wpi, at), False)) * s
    pool_in[...] = pooled.astype(bf)
    head, end = pooled[:REACH], pooled[pooled.shape[0] - REACH :]
    on_first = ids[8] % 2 == 0
    inner = jnp.concatenate([jnp.where(on_first, end, head)] * 2, axis=0).astype(bf)
    q[q.shape[0] - 16 :, :] = jnp.concatenate([inner, inner[:, :128]], axis=1)
    outer[...] = jnp.concatenate([jnp.where(on_first, head, end)] * 2, axis=0).astype(bf)
    lat = (query0[...] + product(n, rows_at(wqd, at), False)) * s
    lat = lat.astype(bf).astype(f32)
    lat = lat * lax.rsqrt(jnp.mean(lat * lat, axis=-1, keepdims=True) + eps) * qgain[...]
    raw = jnp.dot(lat.astype(bf), wqu[...], preferred_element_type=f32)
    raw = jnp.transpose(raw).astype(bf).astype(f32)
    for h in range(raw.shape[0] // HEAD):
        v = raw[h * HEAD : (h + 1) * HEAD]
        v = v * lax.rsqrt(jnp.mean(v * v, axis=0, keepdims=True) + eps) * hgain
        v = v * (HEAD**-0.5 / math.log(2.0))
        first, second = v[NOPE : NOPE + 16], v[NOPE + 16 :]
        base = h * HEAD
        q[base : base + NOPE, :] = v[:NOPE].astype(bf)
        q[base + NOPE : base + NOPE + 16, :] = (first * cos[...] - second * sin[...]).astype(bf)
        q[base + NOPE + 16 : base + HEAD, :] = (first * sin[...] + second * cos[...]).astype(bf)


def gate_kernel(ids, x0, x1a, x1b, x2a, x2b, xa, xb, gain, wa, wp, scale, gate_a, gate_p):
    ns, ats = all_pieces(ids, x0, x1a, x1b, x2a, x2b, xa, xb, gain)
    s = scale[:, :1]
    gate_a[...] = jax.nn.sigmoid(summed(ns, wa, ats) * s)
    gate_p[...] = jax.nn.sigmoid(summed(ns, wp, ats) * s)


def join_kernel(a, b, c, d, out):
    width = a.shape[1]
    for i, x in enumerate((a, b, c, d)):
        out[:, i * width : (i + 1) * width] = x[...]


def chosen(ids, packs, kind):
    mine, other = packs
    take_mine = ids[8] % 2 == kind
    return jnp.where(take_mine, mine[:256, :], other[:256, :])


def pool_merge_kernel(ids, pool, attn, own, f1, f2, f3, s1, s2, s3, gate_a, gate_p, out, attn_w):
    total = jnp.dot(pool[...], own[256:, :], preferred_element_type=f32)
    for k, (f, s) in enumerate(((f1, s1), (f2, s2), (f3, s3))):
        p = jnp.concatenate([f[256:, :256], f[256:, 256:]], axis=0)
        total = total + jnp.dot(p, chosen(ids, (f, s), 1), preferred_element_type=f32)
        attn_w[k * 256 : (k + 1) * 256, :] = chosen(ids, (f, s), 0)
    first = lax.dot_general(attn[...], own[:256, :], (((0,), (0,)), ((), ())), preferred_element_type=f32)
    out[...] = gate_p[...] * total + gate_a[...] * first


def pack_kernel(ids, inner, x, outer, mix, scale, wa, wp, pool, own, s1, s2, s3, padded, sum2, sum4, sum8):
    rows = x.shape[0]
    half, length = ids[9], ids[10]
    on_first = ids[8] % 2 == 0
    inner = inner[inner.shape[0] - 16 :, :256][:REACH].astype(f32)
    outer = outer[...][:REACH].astype(f32)
    padded[0:REACH, :] = jnp.where(on_first, outer, inner)
    padded[REACH : REACH + rows, :] = x[...].astype(f32)
    padded[REACH + rows : rows + 2 * REACH, :] = jnp.where(on_first, inner, outer)
    n = rows + 2 * REACH
    padded[n:, :] = sum2[n:, :] = sum4[n:, :] = jnp.zeros((REACH, x.shape[1]), f32)
    sum2[:n, :] = padded[:n, :] + padded[1 : n + 1, :]
    sum4[:n, :] = sum2[:n, :] + sum2[2 : n + 2, :]
    sum8[:n, :] = sum4[:n, :] + sum4[4 : n + 4, :]
    total = sum8[:rows, :] + sum8[REACH : REACH + rows, :]
    total = jnp.where(half == 4, sum8[4 : 4 + rows, :], total)
    total = jnp.where(half == 2, sum4[6 : 6 + rows, :], total)
    total = jnp.where(half == 1, sum2[7 : 7 + rows, :], total)
    at = ids[8] * rows + lax.broadcasted_iota(jnp.int32, (rows, 1), 0)
    count = (jnp.clip(at + half, 0, length) - jnp.clip(at - half, 0, length)).astype(f32)
    mixed = (total / count - padded[REACH : REACH + rows, :]).astype(bf)
    out = (jnp.dot(mixed, mix[...], preferred_element_type=f32) * scale[...]).astype(bf)
    pool[...] = out
    at = pl.multiple_of(ids[4] * 512, 512)
    own[:256, :] = wa[:, pl.ds(at, 512)]
    own[256:, :] = wp[:, pl.ds(at, 512)]
    for d, s in ((1, s1), (2, s2), (3, s3)):
        at = pl.multiple_of(ids[4 + d] * 512, 512)
        s[:256, :] = jnp.where(on_first, wa[:, pl.ds(at, 512)], wp[:, pl.ds(at, 512)])
        s[256:, :256] = out[: rows // 2]
        s[256:, 256:] = out[rows // 2 :]


def attend_kernel(*refs, pieces, seeded):
    q0, q1, up, gains = refs[:4]
    refs = refs[4:]
    gain = gains[LATENT : LATENT + NOPE]
    n_in = sum(len(p) for p in pieces)
    blocks = refs[:n_in]
    refs = refs[n_in:]
    seeds, outs = (refs[:2], refs[2:]) if seeded else ((), refs)
    heads = q0.shape[0] // HEAD
    half = q0.shape[1]
    at = 0
    for number, piece in enumerate(pieces):
        parts = [blocks[at + i] for i in range(len(piece))]
        at += len(piece)
        whole = parts[0][...] if len(parts) == 1 else jnp.concatenate([p[...] for p in parts], axis=0)
        keys = whole.shape[1]
        latent = whole[:LATENT]
        rope = whole[LATENT : LATENT + ROPE].astype(f32)
        square = whole[LATENT + ROPE :].astype(f32)[0:1]
        expanded = lax.dot_general(up[...], latent, (((0,), (0,)), ((), ())), preferred_element_type=f32)
        row = lax.broadcasted_iota(jnp.int32, (16, keys), 0)
        ones = jnp.where(row == 0, 1.0, 0.0).astype(bf)
        for h in range(heads):
            k = expanded[h * 128 : h * 128 + NOPE]
            scale = lax.rsqrt((jnp.sum(k * k, axis=0, keepdims=True) + square) * (1.0 / HEAD) + eps)
            key = jnp.concatenate([(k * gain * scale).astype(bf), (rope * scale).astype(bf)], axis=0)
            query = jnp.concatenate([q[h * HEAD : (h + 1) * HEAD, :] for q in (q0, q1)], axis=1)
            scores = lax.dot_general(key, query, (((0,), (0,)), ((), ())), preferred_element_type=f32)
            weights = jnp.exp2(scores).astype(bf)
            v = jnp.concatenate([expanded[h * 128 + NOPE : (h + 1) * 128].astype(bf), ones], axis=0)
            add = jnp.dot(v, weights, preferred_element_type=f32)
            for i in range(2):
                part = add[:, i * half : (i + 1) * half]
                if number > 0:
                    outs[i][h] += part
                elif seeded:
                    outs[i][h] = (seeds[i][h] + part).astype(outs[i].dtype)
                else:
                    outs[i][h] = part


def attend(q0, q1, up, gains, pieces, seeds, sent_type=f32):
    heads, half = q0.shape[0] // HEAD, q0.shape[1]
    shape = jax.ShapeDtypeStruct((heads, ACC, half), f32)
    arrays = [a for p in pieces for a in p]
    keys = sum(p[0].shape[1] for p in pieces)
    kernel = functools.partial(
        attend_kernel, pieces=[[None] * len(p) for p in pieces], seeded=seeds is not None
    )
    return call(
        kernel,
        None,
        [q0, q1, up, gains, *[resident(a) for a in (*arrays, *(seeds or ()))]],
        [kept(shape), kept(jax.ShapeDtypeStruct(shape.shape, sent_type))],
        keys * heads * 2 * half * 2 * 512,
        mib=28,
        transcendentals=keys * heads * 2 * half,
    )


def finish_kernel(mine, other, out):
    for h in range(mine.shape[0]):
        both = mine[h] + other[h].astype(f32)
        out[h * VALUE_DIM : (h + 1) * VALUE_DIM, :] = (
            both[:VALUE_DIM] / both[VALUE_DIM : VALUE_DIM + 1]
        ).astype(bf)


def merge_kernel(a1, a2, a3, w, gate, rest, out):
    a = jnp.concatenate([a1[...], a2[...], a3[...]], axis=0)
    total = lax.dot_general(a, w[...], (((0,), (0,)), ((), ())), preferred_element_type=f32)
    out[...] = (gate[...] * total + rest[...]).astype(bf)


def resident(x):
    return pltpu.with_memory_space_constraint(x, pltpu.VMEM)


def kept(s):
    return pltpu.VMEM(s.shape, s.dtype)


def call(kernel, ids, ins, shapes, flops, scratch=(), mib=16, transcendentals=0, apart=()):
    first = [] if ids is None else [ids]
    ins = [pltpu.with_memory_space_constraint(x, pltpu.HBM) if i in apart else x for i, x in enumerate(ins)]
    return pl.pallas_call(
        kernel,
        in_specs=[SM] * len(first)
        + [pl.BlockSpec(memory_space=pltpu.HBM) if i in apart else VM for i in range(len(ins))],
        out_specs=jax.tree.map(lambda _: VM, shapes),
        out_shape=shapes,
        scratch_shapes=scratch,
        compiler_params=params(mib),
        cost_estimate=pl.CostEstimate(flops=flops, transcendentals=transcendentals, bytes_accessed=2**20),
    )(*first, *ins)


def whole(
    tokens,
    norm_gain,
    w_query_down,
    query_gain,
    w_query_up,
    w_latent_down,
    latent_gain,
    w_rotary_key,
    w_latent_up,
    query_head_gain,
    key_head_gain,
    w_pool_in,
    w_pool_mix,
    pool_scale,
    w_attn_out,
    w_pool_out,
    w_gate_attn,
    w_gate_pool,
):
    S = jax.ShapeDtypeStruct
    rows = tokens.shape[0]
    heads = w_query_up.shape[1] // HEAD
    length = rows * lax.axis_size("sp")
    here = lax.axis_index("sp")
    t = lax.axis_index("tp")

    top, bottom = tokens[: rows // 2], tokens[rows // 2 :]
    x1a = lax.ppermute(top, "tp", ring(1))
    x2b = lax.ppermute(bottom, "tp", ring(-1))
    x1b = lax.ppermute(bottom, "tp", ring(1))
    x2a = lax.ppermute(top, "tp", ring(-1))
    xa = lax.ppermute(x1a, "tp", ring(1))
    xb = lax.ppermute(x2b, "tp", ring(-1))

    half = ROPE // 2
    freqs = theta ** (-jnp.arange(half, dtype=f32) / half)
    positions = (here * rows + jnp.arange(rows, dtype=jnp.int32)).astype(f32)
    angles = freqs[:, None] * positions[None, :]
    cos, sin = jnp.cos(angles), jnp.sin(angles)
    fixed = jnp.array([0, 3, 1, 2, 0, 1, 2, 3, 0, 0, length], jnp.int32)
    slot = jnp.arange(11, dtype=jnp.int32)
    ids = jnp.where(slot < 8, (fixed + t) & 3, fixed + (slot == 8) * here + (slot == 9) * jnp.left_shift(1, t))
    gains = jnp.concatenate([latent_gain, key_head_gain, query_head_gain, jnp.zeros((64,), f32)])[None, :]
    gain = norm_gain[None, :]
    wr = w_rotary_key.T

    wanted = [w_latent_down, wr, w_query_down, w_pool_in, w_query_up, gain, tokens, cos, sin, query_gain[None, :]]
    wl, wr, wqd, wpi, wqu, gain, x0, cos, sin, qgain, near_gains = [
        resident(x)
        for x in call(
            functools.partial(load_kernel, count=10),
            None, [*wanted, gains, ids], [kept(S(x.shape, x.dtype)) for x in wanted] + [kept(S((512, 1), f32))],
            4 * 10**8, [pltpu.SemaphoreType.DMA((10,))], apart=(*range(10), 11),
        )
    ]
    square, lat0, raw0, query0, pool0 = [
        resident(x)
        for x in call(
            project_kernel,
            ids, [x0, *[resident(x) for x in (x1a, x1b, x2a, x2b)], gain, wl, wr, wqd, wpi],
            [kept(S(s, f32)) for s in ((rows, 128), (rows, LATENT), (ROPE, rows), (rows, 512), (rows, 256))],
            16 * 10**8,
        )
    ]
    pay, scale = call(
        front_kernel,
        ids,
        [resident(xa), resident(xb), gain, wl, wr, square, lat0, raw0, near_gains, cos, sin],
        [kept(S((PAY, rows), bf)), kept(S((rows, 128), f32))],
        3 * 10**8,
    )
    pieces = [tokens, x1a, x1b, x2a, x2b, xa, xb]

    a1 = lax.ppermute(pay, "sp", along(1, False))
    a2 = lax.ppermute(pay, "sp", along(-1, False))
    a3 = lax.ppermute(pay, "sp", along(2, False))

    q, pool_in, outer = call(
        query_kernel,
        ids,
        [resident(xa), resident(xb), gain, wqd, wpi, resident(scale), query0, pool0, qgain,
         wqu, near_gains, cos, sin],
        [S((heads * HEAD + 16, rows), bf), S((rows, 256), bf), S((2 * REACH, 256), bf)],
        10**9,
    )
    q_other = lax.ppermute(q, "sp", SWAP)
    count = lax.axis_size("sp")
    outer = lax.ppermute(outer, "sp", [(i, i - 1 + 2 * (i % 2)) for i in range(1, count - 1)])

    def attend_on(pieces, seeds, name):
        return attend(q, q_other, w_latent_up, near_gains, pieces, seeds, bf if name == "attend_far" else f32)

    line = call(join_kernel, None, [resident(x) for x in (pay, a1, a2, a3)], kept(S((PAY, 4 * rows), bf)), 10**7)
    b1 = lax.ppermute(line, "sp", along(1, True))
    b2 = lax.ppermute(line, "sp", along(-1, True))
    cut = 160
    b3 = lax.ppermute(b1[:cut], "sp", along(1, True))
    b4 = lax.ppermute(b2[cut:], "sp", along(-1, True))

    pool, own_w, *packs = call(
        pack_kernel,
        ids,
        [q_other, pool_in, outer, w_pool_mix[0], pool_scale[None, :], w_attn_out, w_pool_out],
        [S((rows, 256), bf), S((512, 512), bf)] + [S((448, 512), bf)] * 3,
        10**8,
        [pltpu.VMEM((rows + 3 * REACH, 256), f32)] * 4,
    )
    packs = [lax.ppermute(packs[d - 1], "tp", ring(d)) for d in (1, 2, 3)]
    swapped = [lax.ppermute(p, "sp", SWAP) for p in packs]
    weights = [own_w, *packs, *swapped]

    acc = attend_on([[line]], None, "attend_line")
    acc = attend_on([[b1], [b2]], acc, "attend_near")
    acc = attend_on([[b3, b4]], acc, "attend_far")

    gate_attn, gate_pool = call(
        gate_kernel,
        ids,
        [*pieces, norm_gain[None, :], w_gate_attn, w_gate_pool, scale],
        [kept(S((rows, 512), f32))] * 2,
        5 * 10**8,
    )
    other = lax.ppermute(acc[1], "sp", SWAP)
    attn = call(finish_kernel, None, [resident(acc[0]), resident(other)], kept(S((heads * VALUE_DIM, rows), bf)), 10**7)
    attns = [attn] + [lax.ppermute(attn, "tp", ring(d)) for d in (1, 2, 3)]
    rest, attn_w = call(
        pool_merge_kernel, ids, [pool, attn, *weights, resident(gate_attn), resident(gate_pool)],
        [kept(S((rows, 512), f32)), kept(S((768, 512), bf))], 10**9,
    )
    return call(
        merge_kernel,
        None,
        [*[resident(a) for a in attns[1:]], resident(attn_w), resident(gate_attn), resident(rest)],
        S((rows, 512), bf), 10**9,
    )


def solution(mesh):
    placed = (
        P("sp", "tp"),
        P(),
        P(),
        P(),
        P(None, "tp"),
        P(),
        P(),
        P(),
        P(None, "tp"),
        P(),
        P(),
        P(None, "tp"),
        P("tp", None, None),
        P("tp"),
        P("tp", None),
        P("tp", None),
        P(None, "tp"),
        P(None, "tp"),
    )
    return jax.shard_map(whole, mesh=mesh, in_specs=placed, out_specs=P("sp", "tp"), check_vma=False)
```
